256 devices in a mesh: kv: 32 (over z, y), tp: 8 (over x, core).
Axes of the slice: x: 4, y: 4, z: 8, core: 2. Of those that a mesh axis runs over, the one named last changes fastest.
Arguments:
- hidden_rows: bfloat16 [512, 4096], P('kv', 'tp'), may hold values from -16 to 16
- carried_state: float32 [512, 524288], P('kv', 'tp'), may hold values from -6 to 6
- norm_gain: bfloat16 [4096], replicated, may hold values from 0.099609375 to 1.8984375
- w_query: bfloat16 [4096, 2048], P('kv', 'tp'), may hold values from -0.09375 to 0.09375
- w_key: bfloat16 [4096, 2048], P('kv', 'tp'), may hold values from -0.09375 to 0.09375
- w_decay: bfloat16 [4096, 2048], P('kv', 'tp'), may hold values from -0.375 to 0.375
- w_value: bfloat16 [4096, 4096], P('kv', 'tp'), may hold values from -0.09375 to 0.09375
- w_gate: bfloat16 [4096, 4096], P('kv', 'tp'), may hold values from -0.09375 to 0.09375
- decay_bias: float32 [2048], P('tp'), may hold values from -32 to 8
- head_gain: bfloat16 [256], replicated, may hold values from 0.099609375 to 1.8984375
- w_out: bfloat16 [4096, 4096], P('tp', 'kv'), may hold values from -0.09375 to 0.09375
- mlp_gain: bfloat16 [4096], P('tp'), may hold values from 0.099609375 to 1.8984375
- w_up: bfloat16 [4096, 16384], P('tp', 'kv'), may hold values from -0.09375 to 0.09375
- w_down: bfloat16 [16384, 4096], P('kv', 'tp'), may hold values from -0.046875 to 0.046875
Outputs:
- updated_rows: bfloat16 [512, 4096], P('kv', 'tp')
- new_state: float32 [512, 524288], P('kv', 'tp')
The draws below stay inside these ranges and needn't reach their ends.
All inputs are finite; a program needn't handle non-finite values.
Results may differ from the reference program's by a relative error of at most 0.025.
Values may be sent and summed in bfloat16 or wider, within the bound.
A program may use at most 64 MiB of HBM per device.

```python
import jax
import jax.numpy as jnp
from jax import lax

D = 4096
HEADS = 16
DK = 128
DV = 256
FF = 16384
BATCH = 512
N_TP = 8


def draw_hidden_rows(key, part):
    key_base = jax.random.fold_in(key, 11)
    key_rough = jax.random.fold_in(key, 12)
    columns = jnp.arange(D, dtype=jnp.float32)
    rising = 0.5 * jnp.power(4.0, columns / D)
    rough = jnp.exp(jax.random.uniform(key_rough, (D,), jnp.float32, -0.35, 0.35))
    base = jnp.clip(jax.random.normal(key_base, (BATCH, D), jnp.float32), -5.0, 5.0)
    return (base * rising[None, :] * rough[None, :]).astype(jnp.bfloat16)


def shard_levels(rng, shape, pieces, smallest, largest):
    factor_of, own = 1.0, jax.random.fold_in(rng, 6)
    for dim, blocks in pieces:
        draws = jnp.exp(jax.random.uniform(jax.random.fold_in(own, dim), (blocks,), jnp.float32, smallest / len(pieces), largest / len(pieces)))
        factor_of = factor_of * jnp.repeat(draws, shape[dim] // blocks).reshape([-1 if axis == dim else 1 for axis in range(len(shape))])
    return factor_of


def normal_values(key, shape, deviation, bound, split=(), kind=jnp.bfloat16):
    entries = jax.random.normal(key, shape, jnp.float32) * deviation
    if len(split) > 0:
        entries = shard_levels(key, shape, split, -0.22, 0.18) * entries
    return jnp.clip(entries, min=-bound, max=bound).astype(kind)


def setup_inputs(seed: int = 0) -> dict:
    keys = jax.random.split(jax.random.key(seed), 15)
    hidden_rows = draw_hidden_rows(jax.random.fold_in(keys[14], 71), 0)
    carried_state = normal_values(keys[1], (BATCH, HEADS * DK * DV), 1.0, 6.0, ((0, 32), (1, 8)), jnp.float32)
    norm_gain = jnp.clip(1.0 + 0.18 * jax.random.normal(keys[2], (D,), jnp.float32), 0.099609375, 1.8984375).astype(jnp.bfloat16)
    w_query = normal_values(keys[3], (D, HEADS * DK), D ** -0.5, 0.09375, ((0, 32), (1, 8)))
    w_key = normal_values(keys[4], (D, HEADS * DK), D ** -0.5, 0.09375, ((0, 32), (1, 8)))
    w_decay = normal_values(keys[5], (D, HEADS * DK), (D // 16) ** -0.5, 0.375, ((0, 32), (1, 8)))
    w_value = normal_values(keys[6], (D, HEADS * DV), D ** -0.5, 0.09375, ((0, 32), (1, 8)))
    w_gate = normal_values(keys[7], (D, HEADS * DV), D ** -0.5, 0.09375, ((0, 32), (1, 8)))
    decay_bias = jnp.clip(-32.0 + 40.0 * jax.random.uniform(keys[8], (HEADS * DK,), jnp.float32) ** shard_levels(keys[8], (HEADS * DK,), ((0, 8),), -0.2, 0.2), -32.0, 8.0)
    head_gain = jnp.clip(1.0 + 0.18 * jax.random.normal(keys[9], (DV,), jnp.float32), 0.099609375, 1.8984375).astype(jnp.bfloat16)
    w_out = normal_values(keys[10], (HEADS * DV, D), (HEADS * DV) ** -0.5, 0.09375, ((0, 8), (1, 32)))
    mlp_gain = jnp.clip(1.0 + 0.18 * jax.random.normal(keys[11], (D,), jnp.float32), 0.099609375, 1.8984375).astype(jnp.bfloat16)
    w_up = normal_values(keys[12], (D, FF), D ** -0.5, 0.09375, ((0, 8), (1, 32)))
    w_down = normal_values(keys[13], (FF, D), FF ** -0.5, 0.046875, ((0, 32), (1, 8)))
    return dict(hidden_rows=hidden_rows, carried_state=carried_state, norm_gain=norm_gain, w_query=w_query, w_key=w_key, w_decay=w_decay, w_value=w_value, w_gate=w_gate, decay_bias=decay_bias, head_gain=head_gain, w_out=w_out, mlp_gain=mlp_gain, w_up=w_up, w_down=w_down)


epsilon = 1e-06
decay_normalizer = 16.0

def reference(hidden_rows, carried_state, norm_gain, w_query, w_key, w_decay, w_value, w_gate, decay_bias, head_gain, w_out, mlp_gain, w_up, w_down):
    batch_rows = hidden_rows.shape[0]
    inputs = hidden_rows.astype(jnp.float32)
    normed = (inputs * lax.rsqrt(lax.optimization_barrier(jnp.mean(inputs * inputs, axis=-1, keepdims=True)) + epsilon) * norm_gain.astype(jnp.float32)).astype(jnp.bfloat16)
    queries = jnp.dot(normed, w_query, preferred_element_type=jnp.float32).astype(jnp.bfloat16)
    keys_new = jnp.dot(normed, w_key, preferred_element_type=jnp.float32).astype(jnp.bfloat16)
    decay_pre = jnp.dot(normed, w_decay, preferred_element_type=jnp.float32).astype(jnp.bfloat16)
    values = jnp.dot(normed, w_value, preferred_element_type=jnp.float32).astype(jnp.bfloat16)
    out_gate = jnp.dot(normed, w_gate, preferred_element_type=jnp.float32).astype(jnp.bfloat16)
    log_decay = jax.nn.log_sigmoid(decay_pre.astype(jnp.float32) + decay_bias) / decay_normalizer
    log_decay = log_decay.reshape(batch_rows, HEADS, DK)
    carried = carried_state.reshape(batch_rows, HEADS, DK, DV)
    key_heads = keys_new.astype(jnp.float32).reshape(batch_rows, HEADS, DK)
    value_heads = values.astype(jnp.float32).reshape(batch_rows, HEADS, DV)
    new_state = jnp.exp(log_decay)[..., None] * carried + key_heads[..., None] * value_heads[..., None, :]
    query_heads = queries.astype(jnp.float32).reshape(batch_rows, HEADS, DK) * DK ** (-0.5)
    head_out = jnp.einsum('bhk,bhkv->bhv', query_heads, new_state, precision=lax.Precision.HIGHEST)
    gate_heads = out_gate.astype(jnp.float32).reshape(batch_rows, HEADS, DV)
    mixed = head_out * lax.rsqrt(lax.optimization_barrier(jnp.mean(head_out * head_out, axis=-1, keepdims=True)) + epsilon)
    mixed = (mixed * head_gain.astype(jnp.float32) * jax.nn.silu(gate_heads)).astype(jnp.bfloat16)
    mixed = mixed.reshape(batch_rows, HEADS * DV)
    group_rows = HEADS * DV // N_TP
    attn_total = jnp.zeros((batch_rows, D), jnp.float32)
    for block in range(N_TP):
        low = block * group_rows
        piece = jnp.dot(mixed[:, low:low + group_rows], w_out[low:low + group_rows], preferred_element_type=jnp.float32).astype(jnp.bfloat16)
        piece = lax.optimization_barrier(piece)
        attn_total = attn_total + piece.astype(jnp.float32)
    attn_out = attn_total.astype(jnp.bfloat16)
    residual = (inputs + attn_out.astype(jnp.float32)).astype(jnp.bfloat16)
    resid_float = residual.astype(jnp.float32)
    row_scale = lax.rsqrt(lax.optimization_barrier(jnp.mean(resid_float * resid_float, axis=-1, keepdims=True)) + epsilon)
    mlp_input = (resid_float * row_scale * mlp_gain.astype(jnp.float32)).astype(jnp.bfloat16)
    feature_block = D // N_TP
    up_sum = jnp.zeros((batch_rows, FF), jnp.float32)
    for block in range(N_TP):
        low = block * feature_block
        piece = jnp.dot(mlp_input[:, low:low + feature_block], w_up[low:low + feature_block], preferred_element_type=jnp.float32).astype(jnp.bfloat16)
        piece = lax.optimization_barrier(piece)
        up_sum = up_sum + piece.astype(jnp.float32)
    activation = jnp.square(jax.nn.relu(up_sum)).astype(jnp.bfloat16)
    mlp_out = jnp.dot(activation, w_down, preferred_element_type=jnp.float32).astype(jnp.bfloat16)
    updated_rows = (resid_float + mlp_out.astype(jnp.float32)).astype(jnp.bfloat16)
    return (updated_rows, new_state.reshape(batch_rows, HEADS * DK * DV))
```

```python
import jax
import jax.numpy as jnp
from jax import lax
from jax.experimental import pallas as pl
from jax.experimental.pallas import tpu as pltpu
from jax.sharding import Mesh
from jax.sharding import PartitionSpec as P

D = 4096
DK = 128
DV = 256
EPS = 1e-06
MESH = pl.DeviceIdType.MESH
F32 = jnp.float32
BF16 = jnp.bfloat16
KV = ("z", "y")
TP = ("x", "c")
NZ, NY, NX, NC = 8, 4, 4, 2
NEAR = (0, 1, 7, 2, 6, 3, 5, 4)
FAR = NEAR[::-1]


def place():
    return tuple(lax.axis_index(name) for name in ("z", "y", "x", "c"))


def send(src, dst, sent, arrived, device):
    pltpu.make_async_remote_copy(
        src_ref=src, dst_ref=dst, send_sem=sent, recv_sem=arrived, device_id=device, device_id_type=MESH
    ).start()


def wait(ref, sem):
    pltpu.make_async_copy(ref, ref, sem).wait()


def greet(peers):
    barrier = pltpu.get_barrier_semaphore()
    for device in peers:
        pl.semaphore_signal(barrier, inc=1, device_id=device, device_id_type=MESH)
    pl.semaphore_wait(barrier, len(peers))


def around(index, step, count):
    return lax.rem(index + step, count)


def project_kernel(
    hid, gain, wq, wk, wd, wv, wg, wo, proj, wog,
    hx, sq, xb, wb, pb, rb,
    hx_s, hx_r, sq_s, sq_r, zb_s, zb_r, yb_s, yb_r, db_r, wb_s, wb_r, wo_s, wo_r, rb_s, rb_r,
):
    z, y, x, c = place()
    kv = NY * z + y
    tp = NC * x + c
    h = hid[...].astype(F32)
    hx[x] = (h * gain[pl.ds(tp, 1), :]).astype(BF16)
    sq[tp] = jnp.broadcast_to(jnp.sum(h * h, axis=-1, keepdims=True), (16, 128))
    peers = []
    for dz in range(NZ):
        for dy in range(NY):
            if dz or dy:
                peers.append({"z": around(z, dz, NZ), "y": around(y, dy, NY)})
        if dz:
            peers.append({"z": around(z, dz, NZ), "c": 1 - c})
    for dx in range(NX):
        for dc in range(NC):
            if dx or dc:
                peers.append({"x": around(x, dx, NX), "c": around(c, dc, NC)})
    greet(peers)

    for dx in (2, 1, 3):
        send(hx.at[x], hx.at[x], hx_s, hx_r.at[x], {"x": around(x, dx, NX)})
    for dx in range(NX):
        for dc in range(NC):
            if dx or dc:
                send(sq.at[tp], sq.at[tp], sq_s, sq_r, {"x": around(x, dx, NX), "c": around(c, dc, NC)})

    def slot(origin):
        return wog.at[:, pl.ds(pl.multiple_of(origin * 128, 128), 128)]

    up, down = around(z, 1, NZ), around(z, NZ - 1, NZ)
    send(wo, slot(z), wo_s.at[0], wo_r.at[z], {"z": up})
    send(wo, slot(z), wo_s.at[1], wo_r.at[z], {"z": down})
    wog[:, pl.ds(pl.multiple_of(z * 128, 128), 128)] = wo[...]

    def pass_on(step):
        low = around(z, NZ - step + 1, NZ)
        wait(slot(low), wo_r.at[low])
        send(slot(low), slot(low), wo_s.at[2 * step - 2], wo_r.at[low], {"z": up})
        high = around(z, step - 1, NZ)
        wait(slot(high), wo_r.at[high])
        if step < 4:
            send(slot(high), slot(high), wo_s.at[2 * step - 1], wo_r.at[high], {"z": down})

    mine = pl.ds(pl.multiple_of(0, 128), 128)
    pieces = (
        (0, wv, slice(0, 512)),
        (1, wg, slice(0, 512)),
        (2, wq, slice(0, 256)),
        (2, wk, slice(256, 512)),
        (3, wd, slice(0, 256)),
    )
    for number, (home, array, columns) in enumerate(pieces):
        target = wb.at[y, :, columns]

        @pl.when(y != home)
        def _():
            send(array, target, wb_s.at[number], wb_r, {"y": home})

        @pl.when(y == home)
        def _():
            pltpu.make_async_copy(array, target, wb_r).start()

    def half(ref, number, which):
        return ref.at[number, :, pl.ds(pl.multiple_of(which * 256, 256), 256)]

    for dx in (0, 1, 3, 2):
        xs = around(x, dx, NX)
        if dx:
            wait(hx.at[xs], hx_r.at[xs])
        zt = NC * xs + c
        for dc in range(NC):
            side = around(c, dc, NC)
            src, dst = half(hx, xs, side), half(xb, kv, side)
            if dc:
                send(src, dst, zb_s.at[2 * dx + dc], zb_r.at[z], {"z": zt, "c": side})
            else:

                @pl.when(zt != z)
                def _():
                    send(src, dst, zb_s.at[2 * dx], zb_r.at[z], {"z": zt, "c": side})

                @pl.when(zt == z)
                def _():
                    pltpu.make_async_copy(src, dst, zb_r.at[z]).start()

    pass_on(2)
    for dz in NEAR:
        number = NY * around(z, dz, NZ) + y
        piece = half(xb, number, c)
        wait(piece, zb_r.at[around(z, dz, NZ)])
        for dy in (2, 1, 3):
            send(piece, piece, yb_s, yb_r.at[number], {"y": around(y, dy, NY)})
        send(piece, piece, yb_s, db_r, {"c": 1 - c})
    pass_on(3)
    for dz in NEAR:
        for dy in (1, 3, 2):
            number = NY * around(z, dz, NZ) + around(y, dy, NY)
            piece = half(xb, number, c)
            wait(piece, yb_r.at[number])
            send(piece, piece, yb_s, db_r, {"c": 1 - c})

    @pl.when(y < 3)
    def _():
        wait(wb, wb_r)

    @pl.when(y == 3)
    def _():
        wait(wb.at[:, :, slice(0, 256)], wb_r)

    wait(xb.at[:, :, slice(0, 256)], db_r)
    weights = wb[...].reshape(512, 512)

    def scatter(steps, width):
        for dz in steps:
            zt = around(z, dz, NZ)
            for dy in (2, 1, 3, 0):
                yt = around(y, dy, NY)
                src = pb.at[NY * zt + yt, :, slice(0, width)]
                dst = rb.at[y, z, :, slice(0, width)]
                if dz or dy:
                    send(src, dst, rb_s, rb_r.at[y], {"z": zt, "y": yt})
                else:
                    pltpu.make_async_copy(src, dst, rb_r.at[y]).start()

    groups = (FAR[:4], FAR[4:])
    for number, steps in enumerate(groups):
        rows = [xb[pl.ds(pl.multiple_of(NY * around(z, dz, NZ), NY), NY)].reshape(64, 512) for dz in steps]
        part = jnp.dot(jnp.concatenate(rows, axis=0), weights, preferred_element_type=F32).astype(BF16)
        for place_in, dz in enumerate(steps):
            zt = around(z, dz, NZ)
            pb[pl.ds(pl.multiple_of(NY * zt, NY), NY)] = part[64 * place_in : 64 * place_in + 64].reshape(NY, 16, 512)
        if number == 0:
            pass_on(4)

        @pl.when(y < 3)
        def _():
            scatter(steps, 512)

        @pl.when(y == 3)
        def _():
            scatter(steps, 256)

    wait(sq.at[pl.ds(0, 7)], sq_r)
    scale = lax.rsqrt(jnp.sum(sq[...], axis=0) / D + EPS)[:, 0:1]
    offset = 0
    for block, width in ((3, 256), (2, 512), (0, 512), (1, 512)):
        wait(rb.at[block, :, :, slice(0, width)], rb_r.at[block])
        total = jnp.sum(rb[block, :, :, 0:width].astype(F32), axis=0)
        proj[:, offset : offset + width] = (total * scale).astype(BF16)
        offset += width

    last = around(z, 4, NZ)
    wait(slot(last), wo_r.at[last])
    wait(hx.at[pl.ds(0, 3)], hx_s)
    wait(sq.at[pl.ds(0, 7)], sq_s)
    for number in range(7):
        wait(wo, wo_s.at[number])
    for number, (home, array, columns) in enumerate(pieces):

        @pl.when(y != home)
        def _():
            wait(array, wb_s.at[number])

    for dx in range(NX):
        wait(half(hx, 0, 0), zb_s.at[2 * dx + 1])

        @pl.when(NC * around(x, dx, NX) + c != z)
        def _():
            wait(half(hx, 0, 0), zb_s.at[2 * dx])

    wait(xb.at[pl.ds(0, 28)], yb_s)

    @pl.when(y < 3)
    def _():
        wait(pb.at[pl.ds(0, 31)], rb_s)

    @pl.when(y == 3)
    def _():
        wait(pb.at[pl.ds(0, 31), :, slice(0, 256)], rb_s)


def project(hid, gain, wq, wk, wd, wv, wg, wo):
    dma = pltpu.SemaphoreType.DMA
    vmem = pl.BlockSpec(memory_space=pltpu.VMEM)
    return pl.pallas_call(
        project_kernel,
        out_shape=(jax.ShapeDtypeStruct((16, 1792), BF16), jax.ShapeDtypeStruct((512, 1024), BF16)),
        in_specs=[vmem] * 8,
        out_specs=(vmem, vmem),
        scratch_shapes=[
            pltpu.VMEM((NX, 16, 512), BF16),
            pltpu.VMEM((8, 16, 128), F32),
            pltpu.VMEM((32, 16, 512), BF16),
            pltpu.VMEM((NY, 128, 512), BF16),
            pltpu.VMEM((32, 16, 512), BF16),
            pltpu.VMEM((NY, NZ, 16, 512), BF16),
            dma, dma((NX,)), dma, dma, dma((8,)), dma((NZ,)), dma, dma((32,)), dma,
            dma((5,)), dma, dma((7,)), dma((NZ,)), dma, dma((NY,)),
        ],
        compiler_params=pltpu.CompilerParams(collective_id=0, has_side_effects=True),
        name="project",
    )(hid, gain, wq, wk, wd, wv, wg, wo)


STEPS = 16
WIDE = 65536 // STEPS
KEYS = WIDE // DV


def state_kernel(proj, bias, head_gain, state, new_state, mixed, decay, acc):
    step = pl.program_id(0)
    per_head = DK // KEYS

    @pl.when(step == 0)
    def _():
        pre = proj[:, 0:256].astype(F32) + bias[...]
        soft = jnp.minimum(pre, 0.0) - jnp.log1p(jnp.exp(-jnp.abs(pre)))
        decay[...] = jnp.exp(soft / 16.0)
        acc[...] = jnp.zeros_like(acc)

    head = step // per_head
    back = 256 - step * KEYS
    shift = lax.rem(back, 256)
    rates = pltpu.roll(decay[...], shift, axis=1)
    queries = pltpu.roll(proj[:, 256:512].astype(F32) * DK ** (-0.5), shift, axis=1)
    keys = pltpu.roll(proj[:, 512:768].astype(F32), shift, axis=1)
    columns = pl.ds(pl.multiple_of(head * DV, DV), DV)
    values = proj[:, pl.ds(pl.multiple_of(768 + head * DV, DV), DV)].astype(F32)
    total = acc[:, columns]
    for key in range(KEYS):
        where = slice(key * DV, key * DV + DV)
        fresh = rates[:, key : key + 1] * state[:, where] + keys[:, key : key + 1] * values
        new_state[:, where] = fresh
        total = total + queries[:, key : key + 1] * fresh
    acc[:, columns] = total

    @pl.when(step == STEPS - 1)
    def _():
        for number in range(2):
            part = slice(number * DV, number * DV + DV)
            out = acc[:, part]
            gate = proj[:, 1280 + number * DV : 1280 + number * DV + DV].astype(F32)
            normal = out * lax.rsqrt(jnp.mean(out * out, axis=-1, keepdims=True) + EPS)
            silu = gate / (1.0 + jnp.exp(-gate))
            mixed[:, part] = (normal * head_gain[...].astype(F32) * silu).astype(BF16)


def update_state(proj, bias, head_gain, state):
    fixed = lambda *shape: pl.BlockSpec(shape, lambda i: (0,) * len(shape))
    return pl.pallas_call(
        state_kernel,
        grid=(STEPS,),
        out_shape=(jax.ShapeDtypeStruct((16, 65536), F32), jax.ShapeDtypeStruct((16, 512), BF16)),
        in_specs=[fixed(16, 1792), fixed(1, 256), fixed(1, 256), pl.BlockSpec((16, WIDE), lambda i: (0, i))],
        out_specs=(pl.BlockSpec((16, WIDE), lambda i: (0, i)), fixed(16, 512)),
        scratch_shapes=[pltpu.VMEM((16, 256), F32), pltpu.VMEM((16, 512), F32)],
        compiler_params=pltpu.CompilerParams(dimension_semantics=("arbitrary",)),
        name="update_state",
    )(proj, bias, head_gain, state)


def feed_kernel(
    mixed, wog, hid, gain, wu_hbm, wd_hbm, out,
    wu, wd, mb, hp, op, r2, rp, res, sq, upb, dd, us, ur, act, dp, dy_b, zs, zr,
    w_sem, mb_s, mb_r, hp_s, hp_r, op_s, op_r, rz_s, rz_r, ry_s, ry_r, sq_s, sq_r,
    dd_s, dd_r, us_s, us_r, ac_s, ac_r, ad_r, dy_s, dy_r, zr_s, zr_r,
):
    z, y, x, c = place()
    tp = NC * x + c
    pltpu.make_async_copy(wu_hbm, wu, w_sem.at[0]).start()
    pltpu.make_async_copy(wd_hbm, wd, w_sem.at[1]).start()
    mb[y] = mixed[...]
    tps = [
        {"x": around(x, dx, NX), "c": around(c, dc, NC)} for dx in (2, 1, 3, 0) for dc in range(NC) if dx or dc
    ]
    ys = [{"y": around(y, dy, NY)} for dy in (2, 1, 3)]
    zs_far = [{"z": around(z, dz, NZ)} for dz in FAR[:7]]
    greet(tps + ys + zs_far)

    for device in ys:
        send(mb.at[y], mb.at[y], mb_s, mb_r, device)
    for dy in (2, 1, 3):
        yt = around(y, dy, NY)
        columns = pl.ds(pl.multiple_of(yt * 128, 128), 128)
        send(hid.at[:, columns], hp.at[y], hp_s, hp_r, {"y": yt})
    here = pl.ds(pl.multiple_of(y * 128, 128), 128)
    hp[y] = hid[:, here]
    wait(mb.at[pl.ds(0, 3)], mb_r)
    part = jnp.dot(mb[...].reshape(64, 512), wog[...], preferred_element_type=F32).astype(BF16)
    for t in range(8):
        op[t] = part[:, t * 128 : t * 128 + 128]
    r2[tp] = op[tp]
    for device in tps:
        t = NC * device["x"] + device["c"]
        send(op.at[t], r2.at[tp], op_s, op_r, device)
    wait(hp.at[pl.ds(0, 3)], hp_r)
    wait(r2.at[pl.ds(0, 7)], op_r)
    attn = jnp.sum(r2[...].astype(F32), axis=0).astype(BF16).astype(F32)
    rp[...] = (hp[...].reshape(64, 128).astype(F32) + attn).astype(BF16)
    res[z, :, here] = rp[...]
    for device in zs_far:
        send(rp, res.at[z, :, here], rz_s, rz_r.at[z], device)
    for dz in NEAR:
        zt = around(z, dz, NZ)
        piece = res.at[zt, :, here]
        if dz:
            wait(piece, rz_r.at[zt])
        for device in ys:
            send(piece, piece, ry_s, ry_r.at[NY * zt + y], device)

    def arrived(zt):
        for dy in (1, 3, 2):
            yt = around(y, dy, NY)
            piece = res.at[zt, :, pl.ds(pl.multiple_of(yt * 128, 128), 128)]
            wait(piece, ry_r.at[NY * zt + yt])

    rows = pl.ds(pl.multiple_of(y * 16, 16), 16)
    pltpu.make_async_copy(wu_hbm, wu, w_sem.at[0]).wait()
    pair_near = (0, 1, 3, 2)
    first = z // 2
    for dp_ in pair_near:
        i = around(first, dp_, 4)
        arrived(2 * i)
        arrived(2 * i + 1)
        both = res[pl.ds(pl.multiple_of(2 * i, 2), 2)].reshape(128, 512).astype(F32)
        fed = (both * gain[...].astype(F32)).astype(BF16)
        part = jnp.dot(fed, wu[...], preferred_element_type=F32).astype(BF16)
        upb[pl.ds(pl.multiple_of(2 * i, 2), 2)] = part.reshape(2, 64, 512)
        send(upb.at[2 * i + 1 - c], dd.at[i], dd_s, dd_r.at[i], {"c": 1 - c})
        if dp_ == 0:
            own = res[z, rows, :].astype(F32)
            sq[tp] = jnp.broadcast_to(jnp.sum(own * own, axis=-1, keepdims=True), (16, 128))
    for device in tps:
        send(sq.at[tp], sq.at[tp], sq_s, sq_r, device)
    for dp_ in pair_near:
        i = around(first, dp_, 4)
        wait(dd.at[i], dd_r.at[i])
        us[i] = (upb[2 * i + c].astype(F32) + dd[i].astype(F32)).astype(BF16)

        @pl.when(i != x)
        def _():
            send(us.at[i], ur.at[x], us_s, us_r.at[x], {"x": i})

    total = us[x].astype(F32)
    for dx in (1, 3, 2):
        xs = around(x, dx, NX)
        wait(ur.at[xs], us_r.at[xs])
        total = total + ur[xs].astype(F32)
    act[tp] = jnp.square(jnp.maximum(total, 0.0)).astype(BF16)
    for dx in (2, 1, 3):
        send(act.at[tp], act.at[tp], ac_s, ac_r.at[x], {"x": around(x, dx, NX)})
    send(act.at[tp], act.at[tp], ac_s, ad_r.at[x], {"c": 1 - c})
    pltpu.make_async_copy(wd_hbm, wd, w_sem.at[1]).wait()
    for dx in (0, 1, 3, 2):
        xs = around(x, dx, NX)
        if dx:
            piece = act.at[NC * xs + c]
            wait(piece, ac_r.at[xs])
            send(piece, piece, ac_s, ad_r.at[xs], {"c": 1 - c})
    for dx in (0, 1, 3, 2):
        xs = around(x, dx, NX)
        wait(act.at[NC * xs + 1 - c], ad_r.at[xs])
        both = act[pl.ds(pl.multiple_of(2 * xs, 2), 2)].reshape(128, 512)
        part = jnp.dot(both, wd[...], preferred_element_type=F32).astype(BF16)
        dp[pl.ds(pl.multiple_of(2 * xs, 2), 2)] = part.reshape(2, NY, 16, 512)
        for device in ys:
            send(
                dp.at[pl.ds(pl.multiple_of(2 * xs, 2), 2), device["y"]],
                dy_b.at[y, pl.ds(pl.multiple_of(2 * xs, 2), 2)],
                dy_s,
                dy_r.at[xs],
                device,
            )
    for dx in (0, 1, 3, 2):
        xs = around(x, dx, NX)
        two = pl.ds(pl.multiple_of(2 * xs, 2), 2)
        wait(dy_b.at[pl.ds(0, 3), two], dy_r.at[xs])
        total = dp[two, y].astype(F32)
        for dy in (1, 2, 3):
            total = total + dy_b[around(y, dy, NY), two].astype(F32)
        zs[two] = total.astype(BF16)
        for k in range(2):
            j = 2 * xs + k

            @pl.when(j != z)
            def _():
                send(zs.at[j], zr.at[z], zr_s, zr_r, {"z": j})

    zr[z] = zs[z]
    wait(sq.at[pl.ds(0, 7)], sq_r)
    wait(zr.at[pl.ds(0, 7)], zr_r)
    mean = jnp.sum(sq[...], axis=0)[:, 0:1] / D
    squared = 1.0 / (mean + EPS)
    mlp = (jnp.sum(zr[...].astype(F32), axis=0) * squared).astype(BF16).astype(F32)
    out[...] = (res[z, rows, :].astype(F32) + mlp).astype(BF16)

    wait(mb.at[pl.ds(0, 3)], mb_s)
    wait(hp.at[pl.ds(0, 3)], hp_s)
    wait(r2.at[pl.ds(0, 7)], op_s)
    wait(op.at[pl.ds(0, 7)], rz_s)
    wait(res.at[:, :, slice(0, 384)], ry_s)
    wait(sq.at[pl.ds(0, 7)], sq_s)
    wait(dd, dd_s)
    wait(us.at[pl.ds(0, 3)], us_s)
    wait(act.at[pl.ds(0, 7)], ac_s)
    wait(dy_b.at[pl.ds(0, 3)], dy_s)
    wait(zr.at[pl.ds(0, 7)], zr_s)


def feed(mixed, wog, hid, gain, w_up, w_down):
    dma = pltpu.SemaphoreType.DMA
    vmem = pl.BlockSpec(memory_space=pltpu.VMEM)
    anywhere = pl.BlockSpec(memory_space=pl.ANY)
    return pl.pallas_call(
        feed_kernel,
        out_shape=jax.ShapeDtypeStruct((16, 512), BF16),
        in_specs=[vmem] * 4 + [anywhere] * 2,
        out_specs=vmem,
        scratch_shapes=[
            pltpu.VMEM((512, 512), BF16),
            pltpu.VMEM((512, 512), BF16),
            pltpu.VMEM((NY, 16, 512), BF16),
            pltpu.VMEM((NY, 16, 128), BF16),
            pltpu.VMEM((8, 64, 128), BF16),
            pltpu.VMEM((8, 64, 128), BF16),
            pltpu.VMEM((64, 128), BF16),
            pltpu.VMEM((NZ, 64, 512), BF16),
            pltpu.VMEM((8, 16, 128), F32),
            pltpu.VMEM((8, 64, 512), BF16),
            pltpu.VMEM((4, 64, 512), BF16),
            pltpu.VMEM((4, 64, 512), BF16),
            pltpu.VMEM((4, 64, 512), BF16),
            pltpu.VMEM((8, 64, 512), BF16),
            pltpu.VMEM((8, NY, 16, 512), BF16),
            pltpu.VMEM((NY, 8, 16, 512), BF16),
            pltpu.VMEM((8, 16, 512), BF16),
            pltpu.VMEM((NZ, 16, 512), BF16),
            dma((2,)), dma, dma, dma, dma, dma, dma, dma, dma((NZ,)), dma, dma((32,)), dma, dma,
            dma, dma((4,)), dma, dma((4,)), dma, dma((4,)), dma((4,)), dma, dma((4,)), dma, dma,
        ],
        compiler_params=pltpu.CompilerParams(collective_id=1, has_side_effects=True),
        name="feed",
    )(mixed, wog, hid, gain, w_up, w_down)


def body(
    hidden_rows, carried_state, norm_gain, w_query, w_key, w_decay, w_value, w_gate,
    decay_bias, head_gain, w_out, mlp_gain, w_up, w_down,
):
    gains = norm_gain.astype(F32).reshape(8, 512)
    proj, wog = project(hidden_rows, gains, w_query, w_key, w_decay, w_value, w_gate, w_out)
    new_state, mixed = update_state(proj, decay_bias.reshape(1, 256), head_gain.reshape(1, 256), carried_state)
    updated = feed(mixed, wog, hidden_rows, mlp_gain.reshape(1, 512), w_up, w_down)
    return updated, new_state


def solution(mesh):
    finer = Mesh(mesh.devices.reshape(NZ, NY, NX, NC), ("z", "y", "x", "c"))
    placed = (
        P(KV, TP), P(KV, TP), P(), P(KV, TP), P(KV, TP), P(KV, TP), P(KV, TP), P(KV, TP),
        P(TP), P(), P(TP, KV), P(TP), P(TP, KV), P(KV, TP),
    )
    return jax.shard_map(
        body, mesh=finer, in_specs=placed, out_specs=(P(KV, TP), P(KV, TP)), check_vma=False
    )
```

```python
import jax
import jax.numpy as jnp
from jax import lax
from jax.experimental import pallas as pl
from jax.experimental.pallas import tpu as pltpu
from jax.sharding import Mesh
from jax.sharding import PartitionSpec as P

D = 4096
DK = 128
DV = 256
EPS = 1e-06
MESH = pl.DeviceIdType.MESH
F32 = jnp.float32
BF16 = jnp.bfloat16
KV = ("z", "y")
TP = ("x", "c")
NZ, NY, NX, NC = 8, 4, 4, 2
GROUPS = ((0, 1), (7, 2), (6, 3), (5, 4))
PAIRS = (0, 1, 3, 2)
KEYS = 32


def place():
    return tuple(lax.axis_index(name) for name in ("z", "y", "x", "c"))


def send(src, dst, sent, arrived, device):
    pltpu.make_async_remote_copy(
        src_ref=src, dst_ref=dst, send_sem=sent, recv_sem=arrived, device_id=device, device_id_type=MESH
    ).start()


def wait(ref, sem):
    pltpu.make_async_copy(ref, ref, sem).wait()


def greet(peers):
    barrier = pltpu.get_barrier_semaphore()
    for device in peers:
        pl.semaphore_signal(barrier, inc=1, device_id=device, device_id_type=MESH)
    pl.semaphore_wait(barrier, len(peers))


def around(index, step, count):
    return lax.rem(index + step, count)


def layer_kernel(
    hid_hbm, norm_gain_hbm, bias_hbm, head_gain_hbm, mlp_gain_hbm,
    wq, wk, wd, wv, wg, wo, wu_hbm, wdn_hbm, state_hbm,
    out, new_state, hid, norm_gain, bias, head_gain, mlp_gain,
    hx, sq, xb, wb, pb, rb, proj, wog, state, acc, decay,
    wu, wdn, mb, hp, op, r2, res, sq2, upb, dd, us, ur, act, dp, dyb, zs, zr,
    in_sem, hx_s, hx_r, sq_s, sq_r, zb_s, zb_r, yb_s, yb_r, db_r, wb_s, wb_r, wo_s, wo_r, rb_s, rb_r,
    mb_s, mb_r, hp_s, hp_r, op_s, op_r, rz_s, rz_r, ry_s, ry_r, sq2_s, sq2_r,
    dd_s, dd_r, us_s, us_r, ac_s, ac_r, ad_r, dy_s, dy_r, zr_s, zr_r,
):
    z, y, x, c = place()
    kv = NY * z + y
    tp = NC * x + c
    small = (
        (hid_hbm, hid), (norm_gain_hbm, norm_gain), (bias_hbm, bias), (head_gain_hbm, head_gain), (mlp_gain_hbm, mlp_gain),
    )
    for number, (src, dst) in enumerate(small):
        pltpu.make_async_copy(src, dst, in_sem.at[4 + number]).start()
    pltpu.make_async_copy(state_hbm, state, in_sem.at[0]).start()
    pltpu.make_async_copy(wu_hbm, wu, in_sem.at[1]).start()
    pltpu.make_async_copy(wdn_hbm, wdn, in_sem.at[2]).start()
    for number, (src, dst) in enumerate(small):
        pltpu.make_async_copy(src, dst, in_sem.at[4 + number]).wait()
    h = hid[...].astype(F32)
    gain = norm_gain[pl.ds(pl.multiple_of(tp * 512, 512), 512)].astype(F32).reshape(1, 512)
    hx[x] = (h * gain).astype(BF16)
    sq[tp] = jnp.broadcast_to(jnp.sum(h * h, axis=-1, keepdims=True), (16, 128))
    tps = [
        {"x": around(x, dx, NX), "c": around(c, dc, NC)} for dx in (2, 1, 3, 0) for dc in range(NC) if dx or dc
    ]
    ys = [{"y": around(y, dy, NY)} for dy in (2, 1, 3)]
    zfar = [{"z": around(z, dz, NZ)} for dz in (4, 3, 5, 2, 6, 1, 7)]
    greet(tps + zfar + [{"z": device["z"], "c": 1 - c} for device in zfar] + ys)

    def lanes(index, width):
        return pl.ds(pl.multiple_of(index * width, width), width)

    def slot(origin):
        return wog.at[:, lanes(origin, 128)]

    for dx in (2, 1, 3):
        send(hx.at[x], hx.at[x], hx_s, hx_r.at[x], {"x": around(x, dx, NX)})
    for device in tps:
        send(sq.at[tp], sq.at[tp], sq_s, sq_r, device)
    up, down = around(z, 1, NZ), around(z, NZ - 1, NZ)
    send(wo, slot(z), wo_s.at[0], wo_r.at[z], {"z": up})
    send(wo, slot(z), wo_s.at[1], wo_r.at[z], {"z": down})
    pltpu.make_async_copy(wo, slot(z), in_sem.at[3]).start()
    pieces = (
        (0, wv, slice(0, 512)),
        (1, wg, slice(0, 512)),
        (2, wq, slice(0, 256)),
        (2, wk, slice(256, 512)),
        (3, wd, slice(0, 256)),
    )
    for number, (home, array, columns) in enumerate(pieces):
        target = wb.at[y, :, columns]

        @pl.when(y != home)
        def _():
            send(array, target, wb_s.at[number], wb_r, {"y": home})

        @pl.when(y == home)
        def _():
            pltpu.make_async_copy(array, target, wb_r).start()

    for dy in (2, 1, 3):
        yt = around(y, dy, NY)
        send(hid.at[:, lanes(yt, 128)], hp.at[y], hp_s, hp_r, {"y": yt})
    hp[y] = hid[:, lanes(y, 128)]

    def pass_on(step):
        low = around(z, NZ - step + 1, NZ)
        wait(slot(low), wo_r.at[low])
        send(slot(low), slot(low), wo_s.at[2 * step - 2], wo_r.at[low], {"z": up})
        high = around(z, step - 1, NZ)
        wait(slot(high), wo_r.at[high])
        if step < 4:
            send(slot(high), slot(high), wo_s.at[2 * step - 1], wo_r.at[high], {"z": down})

    def half(ref, number, which):
        return ref.at[number, :, lanes(which, 256)]

    for dx in (0, 1, 3, 2):
        xs = around(x, dx, NX)
        if dx:
            wait(hx.at[xs], hx_r.at[xs])
        zt = NC * xs + c
        for dc in range(NC):
            side = around(c, dc, NC)
            src, dst = half(hx, xs, side), half(xb, kv, side)
            if dc:
                send(src, dst, zb_s.at[2 * dx + dc], zb_r.at[z], {"z": zt, "c": side})
            else:

                @pl.when(zt != z)
                def _():
                    send(src, dst, zb_s.at[2 * dx], zb_r.at[z], {"z": zt, "c": side})

                @pl.when(zt == z)
                def _():
                    pltpu.make_async_copy(src, dst, zb_r.at[z]).start()

    def spread_y(group):
        for dz in group:
            zt = around(z, dz, NZ)
            number = NY * zt + y
            piece = half(xb, number, c)
            wait(piece, zb_r.at[zt])
            for device in ys:
                send(piece, piece, yb_s, yb_r.at[number], device)
            send(piece, piece, yb_s, db_r.at[zt], {"c": 1 - c})

    def spread_c(group):
        for dz in group:
            zt = around(z, dz, NZ)
            for dy in (1, 3, 2):
                number = NY * zt + around(y, dy, NY)
                piece = half(xb, number, c)
                wait(piece, yb_r.at[number])
                send(piece, piece, yb_s, db_r.at[zt], {"c": 1 - c})

    def scatter(steps, width):
        for dz in steps:
            zt = around(z, dz, NZ)
            for dy in (2, 1, 3, 0):
                yt = around(y, dy, NY)
                src = pb.at[NY * zt + yt, :, slice(0, width)]
                dst = rb.at[y, z, :, slice(0, width)]
                if dz or dy:
                    send(src, dst, rb_s, rb_r.at[y], {"z": zt, "y": yt})
                else:
                    pltpu.make_async_copy(src, dst, rb_r.at[y]).start()

    def multiply(group):
        for dz in group:
            zt = around(z, dz, NZ)
            wait(xb.at[pl.ds(pl.multiple_of(NY * zt, NY), NY), :, slice(0, 256)], db_r.at[zt])
        rows = [xb[pl.ds(pl.multiple_of(NY * around(z, dz, NZ), NY), NY)].reshape(64, 512) for dz in group]
        weights = wb[...].reshape(512, 512)
        part = jnp.dot(jnp.concatenate(rows, axis=0), weights, preferred_element_type=F32).astype(BF16)
        for number, dz in enumerate(group):
            zt = around(z, dz, NZ)
            pb[pl.ds(pl.multiple_of(NY * zt, NY), NY)] = part[64 * number : 64 * number + 64].reshape(NY, 16, 512)

        @pl.when(y < 3)
        def _():
            scatter(group, 512)

        @pl.when(y == 3)
        def _():
            scatter(group, 256)

    for group in GROUPS:
        spread_y(group)
    spread_c(GROUPS[0])
    spread_c(GROUPS[1])
    pass_on(2)

    @pl.when(y < 3)
    def _():
        wait(wb, wb_r)

    @pl.when(y == 3)
    def _():
        wait(wb.at[:, :, slice(0, 256)], wb_r)

    multiply(GROUPS[0])
    spread_c(GROUPS[2])
    multiply(GROUPS[1])
    spread_c(GROUPS[3])
    multiply(GROUPS[2])
    multiply(GROUPS[3])
    pass_on(3)

    wait(sq.at[pl.ds(0, 7)], sq_r)
    scale = lax.rsqrt(jnp.sum(sq[...], axis=0) / D + EPS)[:, 0:1]

    def summed(block, width, offset):
        wait(rb.at[block, :, :, slice(0, width)], rb_r.at[block])
        total = jnp.sum(rb[block, :, :, 0:width].astype(F32), axis=0)
        proj[:, offset : offset + width] = (total * scale).astype(BF16).astype(F32)

    summed(3, 256, 0)
    summed(2, 512, 256)
    summed(0, 512, 768)
    summed(1, 512, 1280)
    pre = proj[:, 0:256] + bias[...].reshape(1, 256)
    soft = jnp.minimum(pre, 0.0) - jnp.log1p(jnp.exp(-jnp.abs(pre)))
    decay[...] = jnp.exp(soft / 16.0)
    acc[...] = jnp.zeros_like(acc)
    pltpu.make_async_copy(state_hbm, state, in_sem.at[0]).wait()

    @pl.loop(0, 256 // KEYS)
    def _(step):
        shift = lax.rem(256 - step * KEYS, 256)
        rates = pltpu.roll(decay[...], shift, axis=1)
        queries = pltpu.roll(proj[:, 256:512] * DK ** (-0.5), shift, axis=1)
        keys = pltpu.roll(proj[:, 512:768], shift, axis=1)
        head = step // (DK // KEYS)
        columns = lanes(head, DV)
        values = proj[:, pl.ds(pl.multiple_of(768 + head * DV, DV), DV)]
        total = acc[:, columns]
        for key in range(KEYS):
            where = pl.ds(pl.multiple_of((step * KEYS + key) * DV, DV), DV)
            fresh = rates[:, key : key + 1] * state[:, where] + keys[:, key : key + 1] * values
            new_state[:, where] = fresh
            total = total + queries[:, key : key + 1] * fresh
        acc[:, columns] = total

    for number in range(2):
        part = slice(number * DV, number * DV + DV)
        value = acc[:, part]
        gate = proj[:, 1280 + number * DV : 1280 + number * DV + DV]
        normal = value * lax.rsqrt(jnp.mean(value * value, axis=-1, keepdims=True) + EPS)
        silu = gate / (1.0 + jnp.exp(-gate))
        mb[y, :, part] = (normal * head_gain[...].astype(F32).reshape(1, DV) * silu).astype(BF16)
    for device in ys:
        send(mb.at[y], mb.at[y], mb_s, mb_r, device)
    pass_on(4)
    here = lanes(y, 128)
    last = around(z, 4, NZ)
    wait(slot(last), wo_r.at[last])
    pltpu.make_async_copy(wo, slot(z), in_sem.at[3]).wait()
    wait(mb.at[pl.ds(0, 3)], mb_r)
    part = jnp.dot(mb[...].reshape(64, 512), wog[...], preferred_element_type=F32).astype(BF16)
    for t in range(8):
        op[t] = part[:, t * 128 : t * 128 + 128]
    r2[tp] = op[tp]
    for device in tps:
        t = NC * device["x"] + device["c"]
        send(op.at[t], r2.at[tp], op_s, op_r, device)
    wait(hp.at[pl.ds(0, 3)], hp_r)
    wait(r2.at[pl.ds(0, 7)], op_r)
    attn = jnp.sum(r2[...].astype(F32), axis=0).astype(BF16).astype(F32)
    res[z, :, here] = (hp[...].reshape(64, 128).astype(F32) + attn).astype(BF16)
    mine = res.at[z, :, here]
    for device in zfar:
        send(mine, mine, rz_s, rz_r.at[z], device)
    for device in ys:
        send(mine, mine, ry_s, ry_r.at[kv], device)

    rows = pl.ds(pl.multiple_of(y * 16, 16), 16)
    first = z // 2

    def two(pair):
        return pl.ds(pl.multiple_of(2 * pair, 2), 2)

    def relay(pair):
        for k in range(2):
            zt = 2 * pair + k
            piece = res.at[zt, :, here]

            @pl.when(zt != z)
            def _():
                wait(piece, rz_r.at[zt])
                for device in ys:
                    send(piece, piece, ry_s, ry_r.at[NY * zt + y], device)

    def raise_up(pair):
        for k in range(2):
            zt = 2 * pair + k
            for dy in (1, 3, 2):
                yt = around(y, dy, NY)
                wait(res.at[zt, :, lanes(yt, 128)], ry_r.at[NY * zt + yt])
        both = res[two(pair)].reshape(128, 512).astype(F32)
        fed = (both * mlp_gain[...].astype(F32).reshape(1, 512)).astype(BF16)
        part = jnp.dot(fed, wu[...], preferred_element_type=F32).astype(BF16)
        upb[two(pair)] = part.reshape(2, 64, 512)
        send(upb.at[2 * pair + 1 - c], dd.at[pair], dd_s, dd_r.at[pair], {"c": 1 - c})

    def squares():
        own = res[z, rows, :].astype(F32)
        sq2[tp] = jnp.broadcast_to(jnp.sum(own * own, axis=-1, keepdims=True), (16, 128))
        for device in tps:
            send(sq2.at[tp], sq2.at[tp], sq2_s, sq2_r, device)

    def across(pair):
        wait(dd.at[pair], dd_r.at[pair])
        us[pair] = (upb[2 * pair + c].astype(F32) + dd[pair].astype(F32)).astype(BF16)

        @pl.when(pair != x)
        def _():
            send(us.at[pair], ur.at[x], us_s, us_r.at[x], {"x": pair})

    def activate(pair):
        @pl.when(pair == x)
        def _():
            total = us[x].astype(F32)
            for dx in (1, 3, 2):
                xs = around(x, dx, NX)
                wait(ur.at[xs], us_r.at[xs])
                total = total + ur[xs].astype(F32)
            act[tp] = jnp.square(jnp.maximum(total, 0.0)).astype(BF16)
            for dx in (2, 1, 3):
                send(act.at[tp], act.at[tp], ac_s, ac_r.at[x], {"x": around(x, dx, NX)})
            send(act.at[tp], act.at[tp], ac_s, ad_r.at[x], {"c": 1 - c})

    def hand_over(pair):
        @pl.when(pair != x)
        def _():
            piece = act.at[NC * pair + c]
            wait(piece, ac_r.at[pair])
            send(piece, piece, ac_s, ad_r.at[pair], {"c": 1 - c})

    def bring_down(pair):
        wait(act.at[NC * pair + 1 - c], ad_r.at[pair])
        part = jnp.dot(act[two(pair)].reshape(128, 512), wdn[...], preferred_element_type=F32).astype(BF16)
        dp[two(pair)] = part.reshape(2, NY, 16, 512)
        for device in ys:
            send(dp.at[two(pair), device["y"]], dyb.at[y, two(pair)], dy_s, dy_r.at[pair], device)

    def settle(pair):
        wait(dyb.at[pl.ds(0, 3), two(pair)], dy_r.at[pair])
        total = dp[two(pair), y].astype(F32)
        for dy in (1, 2, 3):
            total = total + dyb[around(y, dy, NY), two(pair)].astype(F32)
        zs[two(pair)] = total.astype(BF16)
        for k in range(2):
            j = 2 * pair + k

            @pl.when(j != z)
            def _():
                send(zs.at[j], zr.at[z], zr_s, zr_r, {"z": j})

    stages = (
        (0.0, relay), (2.0, raise_up), (3.1, across), (5.2, activate), (7.3, hand_over), (8.1, bring_down), (10.5, settle),
    )
    order = sorted((offset + turn, stage, turn) for stage, (offset, _) in enumerate(stages) for turn in range(4))
    pltpu.make_async_copy(wu_hbm, wu, in_sem.at[1]).wait()
    pltpu.make_async_copy(wdn_hbm, wdn, in_sem.at[2]).wait()
    for _, stage, turn in order:
        stages[stage][1](around(first, PAIRS[turn], 4))
        if stage == 1 and turn == 0:
            squares()

    zr[z] = zs[z]
    wait(sq2.at[pl.ds(0, 7)], sq2_r)
    wait(zr.at[pl.ds(0, 7)], zr_r)
    mean = jnp.sum(sq2[...], axis=0)[:, 0:1] / D
    squared = 1.0 / (mean + EPS)
    mlp = (jnp.sum(zr[...].astype(F32), axis=0) * squared).astype(BF16).astype(F32)
    out[...] = (res[z, rows, :].astype(F32) + mlp).astype(BF16)

    wait(hx.at[pl.ds(0, 3)], hx_s)
    wait(sq.at[pl.ds(0, 7)], sq_s)
    for number in range(7):
        wait(slot(0), wo_s.at[number])
    for number, (home, array, columns) in enumerate(pieces):

        @pl.when(y != home)
        def _():
            wait(wb.at[0, :, columns], wb_s.at[number])

    for dx in range(NX):
        wait(half(hx, 0, 0), zb_s.at[2 * dx + 1])

        @pl.when(NC * around(x, dx, NX) + c != z)
        def _():
            wait(half(hx, 0, 0), zb_s.at[2 * dx])

    wait(xb.at[pl.ds(0, 28)], yb_s)

    @pl.when(y < 3)
    def _():
        wait(pb.at[pl.ds(0, 31)], rb_s)

    @pl.when(y == 3)
    def _():
        wait(pb.at[pl.ds(0, 31), :, slice(0, 256)], rb_s)

    wait(mb.at[pl.ds(0, 3)], mb_s)
    wait(hp.at[pl.ds(0, 3)], hp_s)
    wait(r2.at[pl.ds(0, 7)], op_s)
    wait(op.at[pl.ds(0, 7)], rz_s)
    wait(res.at[:, :, slice(0, 384)], ry_s)
    wait(sq2.at[pl.ds(0, 7)], sq2_s)
    wait(dd, dd_s)
    wait(us.at[pl.ds(0, 3)], us_s)
    wait(act.at[pl.ds(0, 7)], ac_s)
    wait(dyb.at[pl.ds(0, 3)], dy_s)
    wait(zr.at[pl.ds(0, 7)], zr_s)


def body(
    hidden_rows, carried_state, norm_gain, w_query, w_key, w_decay, w_value, w_gate,
    decay_bias, head_gain, w_out, mlp_gain, w_up, w_down,
):
    dma = pltpu.SemaphoreType.DMA
    vmem = pl.BlockSpec(memory_space=pltpu.VMEM)
    return pl.pallas_call(
        layer_kernel,
        out_shape=(pltpu.VMEM((16, 512), BF16), pltpu.VMEM((16, 65536), F32)),
        in_specs=[pl.BlockSpec(memory_space=pltpu.HBM)] * 14,
        out_specs=(vmem, vmem),
        scratch_shapes=[
            pltpu.VMEM((16, 512), BF16),
            pltpu.VMEM((4096,), BF16),
            pltpu.VMEM((256,), F32),
            pltpu.VMEM((256,), BF16),
            pltpu.VMEM((512,), BF16),
            pltpu.VMEM((NX, 16, 512), BF16),
            pltpu.VMEM((8, 16, 128), F32),
            pltpu.VMEM((32, 16, 512), BF16),
            pltpu.VMEM((NY, 128, 512), BF16),
            pltpu.VMEM((32, 16, 512), BF16),
            pltpu.VMEM((NY, NZ, 16, 512), BF16),
            pltpu.VMEM((16, 1792), F32),
            pltpu.VMEM((512, 1024), BF16),
            pltpu.VMEM((16, 65536), F32),
            pltpu.VMEM((16, 512), F32),
            pltpu.VMEM((16, 256), F32),
            pltpu.VMEM((512, 512), BF16),
            pltpu.VMEM((512, 512), BF16),
            pltpu.VMEM((NY, 16, 512), BF16),
            pltpu.VMEM((NY, 16, 128), BF16),
            pltpu.VMEM((8, 64, 128), BF16),
            pltpu.VMEM((8, 64, 128), BF16),
            pltpu.VMEM((NZ, 64, 512), BF16),
            pltpu.VMEM((8, 16, 128), F32),
            pltpu.VMEM((8, 64, 512), BF16),
            pltpu.VMEM((4, 64, 512), BF16),
            pltpu.VMEM((4, 64, 512), BF16),
            pltpu.VMEM((4, 64, 512), BF16),
            pltpu.VMEM((8, 64, 512), BF16),
            pltpu.VMEM((8, NY, 16, 512), BF16),
            pltpu.VMEM((NY, 8, 16, 512), BF16),
            pltpu.VMEM((8, 16, 512), BF16),
            pltpu.VMEM((NZ, 16, 512), BF16),
            dma((9,)), dma, dma((NX,)), dma, dma, dma((8,)), dma((NZ,)), dma, dma((32,)), dma((NZ,)),
            dma((5,)), dma, dma((7,)), dma((NZ,)), dma, dma((NY,)),
            dma, dma, dma, dma, dma, dma, dma, dma((NZ,)), dma, dma((32,)), dma, dma,
            dma, dma((4,)), dma, dma((4,)), dma, dma((4,)), dma((4,)), dma, dma((4,)), dma, dma,
        ],
        compiler_params=pltpu.CompilerParams(collective_id=0, has_side_effects=True, vmem_limit_bytes=(59 << 20) + (800 << 10)),
        name="layer",
    )(
        hidden_rows, norm_gain, decay_bias, head_gain, mlp_gain, w_query, w_key, w_decay, w_value, w_gate,
        w_out, w_up, w_down, carried_state,
    )


def solution(mesh):
    finer = Mesh(mesh.devices.reshape(NZ, NY, NX, NC), ("z", "y", "x", "c"))
    placed = (
        P(KV, TP), P(KV, TP), P(), P(KV, TP), P(KV, TP), P(KV, TP), P(KV, TP), P(KV, TP),
        P(TP), P(), P(TP, KV), P(TP), P(TP, KV), P(KV, TP),
    )
    return jax.shard_map(
        body, mesh=finer, in_specs=placed, out_specs=(P(KV, TP), P(KV, TP)), check_vma=False
    )
```

```python
import jax
import jax.numpy as jnp
from jax import lax
from jax.experimental import pallas as pl
from jax.experimental.pallas import tpu as pltpu
from jax.sharding import Mesh
from jax.sharding import PartitionSpec as P

D = 4096
DK = 128
DV = 256
EPS = 1e-06
MESH = pl.DeviceIdType.MESH
F32 = jnp.float32
BF16 = jnp.bfloat16
KV = ("z", "y")
TP = ("x", "c")
NZ, NY, NX, NC = 8, 4, 4, 2
GROUPS = ((0, 1), (7, 2), (6, 3), (5, 4))
PAIRS = (0, 1, 3, 2)
KEYS = 32


def place():
    return tuple(lax.axis_index(name) for name in ("z", "y", "x", "c"))


def send(src, dst, sent, arrived, device):
    pltpu.make_async_remote_copy(
        src_ref=src, dst_ref=dst, send_sem=sent, recv_sem=arrived, device_id=device, device_id_type=MESH
    ).start()


def wait(ref, sem):
    pltpu.make_async_copy(ref, ref, sem).wait()


def greet(peers):
    for device in peers:
        pl.semaphore_signal(pltpu.get_barrier_semaphore(), inc=1, device_id=device, device_id_type=MESH)


def around(index, step, count):
    return lax.rem(index + step, count)


def layer_kernel(
    hid_hbm, norm_gain_hbm, bias_hbm, head_gain_hbm, mlp_gain_hbm,
    wq, wk, wd, wv, wg, wo, wu_hbm, wdn_hbm, state_hbm,
    out, new_state, hid, norm_gain, bias, head_gain, mlp_gain,
    hx, sq, xb, wb, pb, rb, rl, proj, wog, state, acc, decay, asked,
    wu, wdn, mb, hp, op, r2, res, sq2, upb, dd, us, ur, act, dp, dyb, zs, zr,
    in_sem, hx_s, hx_r, sq_s, sq_r, zb_s, zb_r, yb_s, yb_r, db_r, wb_s, wb_r, wo_s, wo_r, rb_s, rb_r, rl_s, rl_r,
    mb_s, mb_r, hp_s, hp_r, op_s, op_r, rz_s, rz_r, ry_s, ry_r, sq2_s, sq2_r,
    dd_s, dd_r, us_s, us_r, ac_s, ac_r, ad_r, dy_s, dy_r, zr_s, zr_r,
):
    z, y, x, c = place()
    kv = NY * z + y
    tp = NC * x + c
    small = (
        (hid_hbm, hid), (norm_gain_hbm, norm_gain), (bias_hbm, bias), (head_gain_hbm, head_gain), (mlp_gain_hbm, mlp_gain),
    )
    for number, (src, dst) in enumerate(small):
        pltpu.make_async_copy(src, dst, in_sem.at[4 + number]).start()
    pltpu.make_async_copy(state_hbm, state, in_sem.at[0]).start()
    pltpu.make_async_copy(wu_hbm, wu, in_sem.at[1]).start()
    pltpu.make_async_copy(wdn_hbm, wdn, in_sem.at[2]).start()
    tps = [
        {"x": around(x, dx, NX), "c": around(c, dc, NC)} for dx in (2, 1, 3, 0) for dc in range(NC) if dx or dc
    ]
    ys = [{"y": around(y, dy, NY)} for dy in (2, 1, 3)]
    zfar = [{"z": around(z, dz, NZ)} for dz in (4, 3, 5, 2, 6, 1, 7)]
    peers = tps + zfar + [{"z": device["z"], "c": 1 - c} for device in zfar] + ys
    greet(peers)
    for number, (src, dst) in enumerate(small):
        pltpu.make_async_copy(src, dst, in_sem.at[4 + number]).wait()
    h = hid[...].astype(F32)
    gain = norm_gain[pl.ds(pl.multiple_of(tp * 512, 512), 512)].astype(F32).reshape(1, 512)
    hx[x] = (h * gain).astype(BF16)
    sq[tp] = jnp.broadcast_to(jnp.sum(h * h, axis=-1, keepdims=True), (16, 128))
    pl.semaphore_wait(pltpu.get_barrier_semaphore(), len(peers))

    def lanes(index, width):
        return pl.ds(pl.multiple_of(index * width, width), width)

    side = 1 - 2 * c

    def at(offset):
        return lax.rem(z + offset * side + NZ, NZ)

    def slot(origin, part):
        return wog.at[pl.ds(part * 256, 256), lanes(origin, 128)]

    for dx in (2, 1, 3):
        send(hx.at[x], hx.at[x], hx_s, hx_r.at[x], {"x": around(x, dx, NX)})
    for device in tps:
        send(sq.at[tp], sq.at[tp], sq_s, sq_r, device)
    up, down = around(z, 1, NZ), around(z, NZ - 1, NZ)
    for part in range(2):
        mine = wo.at[pl.ds(part * 256, 256)]
        send(mine, slot(z, part), wo_s.at[7 * part], wo_r.at[part, z], {"z": up})
        send(mine, slot(z, part), wo_s.at[7 * part + 1], wo_r.at[part, z], {"z": down})
    own_out = pltpu.make_async_copy(wo, wog.at[:, lanes(z, 128)], in_sem.at[3])
    own_out.start()
    pieces = (
        (0, wv, slice(0, 512)),
        (1, wg, slice(0, 512)),
        (2, wq, slice(0, 256)),
        (2, wk, slice(256, 512)),
        (3, wd, slice(0, 256)),
    )
    for number, (home, array, columns) in enumerate(pieces):
        target = wb.at[y, :, columns]

        @pl.when(y != home)
        def _():
            send(array, target, wb_s.at[number], wb_r, {"y": home})

        @pl.when(y == home)
        def _():
            pltpu.make_async_copy(array, target, wb_r).start()

    for dy in (2, 1, 3):
        yt = around(y, dy, NY)
        send(hid.at[:, lanes(yt, 128)], hp.at[y], hp_s, hp_r, {"y": yt})
    hp[y] = hid[:, lanes(y, 128)]

    def pass_on(step, part):
        low = around(z, NZ - step + 1, NZ)
        wait(slot(low, part), wo_r.at[part, low])
        send(slot(low, part), slot(low, part), wo_s.at[7 * part + 2 * step - 2], wo_r.at[part, low], {"z": up})
        high = around(z, step - 1, NZ)
        wait(slot(high, part), wo_r.at[part, high])
        if step < 4:
            send(slot(high, part), slot(high, part), wo_s.at[7 * part + 2 * step - 1], wo_r.at[part, high], {"z": down})

    def half(ref, number, which):
        return ref.at[number, :, lanes(which, 256)]

    for dx in (0, 1, 3, 2):
        xs = around(x, dx, NX)
        if dx:
            wait(hx.at[xs], hx_r.at[xs])
        zt = NC * xs + c
        for dc in range(NC):
            core = around(c, dc, NC)
            src, dst = half(hx, xs, core), half(xb, kv, core)
            if dc:
                send(src, dst, zb_s.at[2 * dx + dc], zb_r.at[z], {"z": zt, "c": core})
            else:

                @pl.when(zt != z)
                def _():
                    send(src, dst, zb_s.at[2 * dx], zb_r.at[z], {"z": zt, "c": core})

                @pl.when(zt == z)
                def _():
                    pltpu.make_async_copy(src, dst, zb_r.at[z]).start()

    def spread_y(group):
        for dz in group:
            zt = at(dz)
            number = NY * zt + y
            piece = half(xb, number, c)
            wait(piece, zb_r.at[zt])
            for device in ys:
                send(piece, piece, yb_s, yb_r.at[number], device)
            send(piece, piece, yb_s, db_r.at[zt], {"c": 1 - c})

    def spread_c(group):
        for dz in group:
            zt = at(dz)
            for dy in (1, 3, 2):
                number = NY * zt + around(y, dy, NY)
                piece = half(xb, number, c)
                wait(piece, yb_r.at[number])
                send(piece, piece, yb_s, db_r.at[zt], {"c": 1 - c})

    def plane(offset):
        return pl.ds(pl.multiple_of(NY * at(offset), NY), NY)

    def by_width(action):
        @pl.when(y < 3)
        def _():
            action(512)

        @pl.when(y == 3)
        def _():
            action(256)

    def scatter(offset, kind, width):
        for dy in (2, 1, 3, 0):
            yt = around(y, dy, NY)
            src = pb.at[NY * at(offset) + yt, :, slice(0, width)]
            dst = rb.at[y, kind, :, slice(0, width)]
            if offset or dy:
                send(src, dst, rb_s, rb_r.at[y], {"z": at(offset), "y": yt})
            else:
                pltpu.make_async_copy(src, dst, rb_r.at[y]).start()

    def lend(offset, number, via, width):
        src, dst = pb.at[plane(offset), :, slice(0, width)], rl.at[number, :, :, slice(0, width)]
        send(src, dst, rl_s, rl_r.at[number], {"z": at(via)})

    def combine(offset, number, kind, width):
        wait(rl.at[number, :, :, slice(0, width)], rl_r.at[number])
        total = pb[plane(offset), :, 0:width].astype(F32) + rl[number, :, :, 0:width].astype(F32)
        pb[plane(offset), :, 0:width] = total.astype(BF16)
        scatter(offset, kind, width)

    def multiply(group):
        for dz in group:
            wait(xb.at[plane(dz), :, slice(0, 256)], db_r.at[at(dz)])
        rows = [xb[plane(dz)].reshape(64, 512) for dz in group]
        weights = wb[...].reshape(512, 512)
        part = jnp.dot(jnp.concatenate(rows, axis=0), weights, preferred_element_type=F32).astype(BF16)
        for number, dz in enumerate(group):
            pb[plane(dz)] = part[64 * number : 64 * number + 64].reshape(NY, 16, 512)

    spread_y(GROUPS[0])
    pass_on(2, 0)
    spread_y(GROUPS[1])
    pass_on(2, 1)
    spread_y(GROUPS[2])
    spread_y(GROUPS[3])
    spread_c(GROUPS[0])
    pass_on(3, 0)
    spread_c(GROUPS[1])
    pass_on(3, 1)
    by_width(lambda width: wait(wb.at[:, :, slice(0, width)], wb_r))
    multiply(GROUPS[0])
    spread_c(GROUPS[2])
    by_width(lambda width: scatter(0, 0, width))
    multiply(GROUPS[1])
    spread_c(GROUPS[3])
    by_width(lambda width: (lend(2, 0, 1, width), scatter(7, 4, width)))
    multiply(GROUPS[3])
    by_width(lambda width: (lend(4, 1, 1, width), lend(5, 2, 7, width)))
    multiply(GROUPS[2])
    by_width(lambda width: combine(1, 0, 1, width))
    pass_on(4, 0)
    by_width(lambda width: combine(3, 1, 2, width))
    by_width(lambda width: combine(6, 2, 3, width))
    pass_on(4, 1)

    wait(sq.at[pl.ds(0, 7)], sq_r)
    scale = lax.rsqrt(jnp.sum(sq[...], axis=0) / D + EPS)[:, 0:1]

    def summed(block, width, offset):
        wait(rb.at[block, :, :, slice(0, width)], rb_r.at[block])
        total = jnp.sum(rb[block, :, :, 0:width].astype(F32), axis=0)
        proj[:, offset : offset + width] = (total * scale).astype(BF16).astype(F32)

    summed(3, 256, 0)
    summed(2, 512, 256)
    summed(0, 512, 768)
    summed(1, 512, 1280)
    pre = proj[:, 0:256] + bias[...].reshape(1, 256)
    soft = jnp.minimum(pre, 0.0) - jnp.log1p(jnp.exp(-jnp.abs(pre)))
    decay[...] = jnp.exp(soft / 16.0)
    acc[...] = jnp.zeros_like(acc)
    queries, keys_now = proj[:, 256:512] * DK ** (-0.5), proj[:, 512:768]
    asked[...] = queries * decay[...]
    for head in range(2):
        columns = slice(head * DK, head * DK + DK)
        meet = jnp.sum(queries[:, columns] * keys_now[:, columns], axis=-1, keepdims=True)
        acc[:, head * DV : head * DV + DV] = meet * proj[:, 768 + head * DV : 768 + head * DV + DV]
    pltpu.make_async_copy(state_hbm, state, in_sem.at[0]).wait()

    def turned(ref, step):
        return pltpu.roll(ref, lax.rem(256 - step * KEYS, 256), axis=1)

    @pl.loop(0, 256 // KEYS)
    def _(step):
        weights = turned(asked[...], step)
        columns = lanes(step // (DK // KEYS), DV)
        totals = [acc[:, columns], jnp.zeros((16, DV), F32)]
        for key in range(KEYS):
            where = pl.ds(pl.multiple_of((step * KEYS + key) * DV, DV), DV)
            totals[key % 2] = totals[key % 2] + weights[:, key : key + 1] * state[:, where]
        acc[:, columns] = totals[0] + totals[1]

    def renew(first_step, steps):
        @pl.loop(first_step, first_step + steps)
        def _(step):
            rates = turned(decay[...], step)
            keys = turned(proj[:, 512:768], step)
            values = proj[:, pl.ds(pl.multiple_of(768 + step // (DK // KEYS) * DV, DV), DV)]
            for key in range(KEYS):
                where = pl.ds(pl.multiple_of((step * KEYS + key) * DV, DV), DV)
                new_state[:, where] = rates[:, key : key + 1] * state[:, where] + keys[:, key : key + 1] * values

    for number in range(2):
        part = slice(number * DV, number * DV + DV)
        value = acc[:, part]
        gate = proj[:, 1280 + number * DV : 1280 + number * DV + DV]
        normal = value * lax.rsqrt(jnp.mean(value * value, axis=-1, keepdims=True) + EPS)
        silu = gate / (1.0 + jnp.exp(-gate))
        mb[y, :, part] = (normal * head_gain[...].astype(F32).reshape(1, DV) * silu).astype(BF16)
    for device in ys:
        send(mb.at[y], mb.at[y], mb_s, mb_r, device)
    renew(0, 2)
    here = lanes(y, 128)
    last = around(z, 4, NZ)
    for part in range(2):
        wait(slot(last, part), wo_r.at[part, last])
    own_out.wait()
    wait(mb.at[pl.ds(0, 3)], mb_r)
    part = jnp.dot(mb[...].reshape(64, 512), wog[...], preferred_element_type=F32).astype(BF16)
    for t in range(8):
        op[t] = part[:, t * 128 : t * 128 + 128]
    r2[tp] = op[tp]
    for device in tps:
        t = NC * device["x"] + device["c"]
        send(op.at[t], r2.at[tp], op_s, op_r, device)
    renew(2, 2)
    wait(hp.at[pl.ds(0, 3)], hp_r)
    wait(r2.at[pl.ds(0, 7)], op_r)
    attn = jnp.sum(r2[...].astype(F32), axis=0).astype(BF16).astype(F32)
    res[z, :, here] = (hp[...].reshape(64, 128).astype(F32) + attn).astype(BF16)
    mine = res.at[z, :, here]
    for device in zfar[::-1]:
        send(mine, mine, rz_s, rz_r.at[z], device)
    for device in ys:
        send(mine, mine, ry_s, ry_r.at[kv], device)

    rows = pl.ds(pl.multiple_of(y * 16, 16), 16)
    first = z // 2
    lean = 2 * (z % 2) - 1

    def two(pair):
        return pl.ds(pl.multiple_of(2 * pair, 2), 2)

    def relay(pair):
        for k in range(2):
            zt = 2 * pair + k
            piece = res.at[zt, :, here]

            @pl.when(zt != z)
            def _():
                wait(piece, rz_r.at[zt])
                for device in ys:
                    send(piece, piece, ry_s, ry_r.at[NY * zt + y], device)

    def raise_up(pair):
        for k in range(2):
            zt = 2 * pair + k
            for dy in (1, 3, 2):
                yt = around(y, dy, NY)
                wait(res.at[zt, :, lanes(yt, 128)], ry_r.at[NY * zt + yt])
        both = res[two(pair)].reshape(128, 512).astype(F32)
        fed = (both * mlp_gain[...].astype(F32).reshape(1, 512)).astype(BF16)
        part = jnp.dot(fed, wu[...], preferred_element_type=F32).astype(BF16)
        upb[two(pair)] = part.reshape(2, 64, 512)
        send(upb.at[2 * pair + 1 - c], dd.at[pair], dd_s, dd_r.at[pair], {"c": 1 - c})

    def squares():
        own = res[z, rows, :].astype(F32)
        sq2[tp] = jnp.broadcast_to(jnp.sum(own * own, axis=-1, keepdims=True), (16, 128))
        for device in tps:
            send(sq2.at[tp], sq2.at[tp], sq2_s, sq2_r, device)

    def across(pair):
        wait(dd.at[pair], dd_r.at[pair])
        us[pair] = (upb[2 * pair + c].astype(F32) + dd[pair].astype(F32)).astype(BF16)

        @pl.when(pair != x)
        def _():
            send(us.at[pair], ur.at[x], us_s, us_r.at[x], {"x": pair})

    def activate(pair):
        @pl.when(pair == x)
        def _():
            total = us[x].astype(F32)
            for dx in (1, 3, 2):
                xs = around(x, dx, NX)
                wait(ur.at[xs], us_r.at[xs])
                total = total + ur[xs].astype(F32)
            act[tp] = jnp.square(jnp.maximum(total, 0.0)).astype(BF16)
            for dx in (2, 1, 3):
                send(act.at[tp], act.at[tp], ac_s, ac_r.at[x], {"x": around(x, dx, NX)})
            send(act.at[tp], act.at[tp], ac_s, ad_r.at[x], {"c": 1 - c})

    def hand_over(pair):
        @pl.when(pair != x)
        def _():
            piece = act.at[NC * pair + c]
            wait(piece, ac_r.at[pair])
            send(piece, piece, ac_s, ad_r.at[pair], {"c": 1 - c})

    def bring_down(pair):
        wait(act.at[NC * pair + 1 - c], ad_r.at[pair])
        part = jnp.dot(act[two(pair)].reshape(128, 512), wdn[...], preferred_element_type=F32).astype(BF16)
        dp[two(pair)] = part.reshape(2, NY, 16, 512)
        for device in ys:
            send(dp.at[two(pair), device["y"]], dyb.at[y, two(pair)], dy_s, dy_r.at[pair], device)

    def settle(pair):
        wait(dyb.at[pl.ds(0, 3), two(pair)], dy_r.at[pair])
        total = dp[two(pair), y].astype(F32)
        for dy in (1, 2, 3):
            total = total + dyb[around(y, dy, NY), two(pair)].astype(F32)
        zs[two(pair)] = total.astype(BF16)
        for k in range(2):
            j = 2 * pair + k

            @pl.when(j != z)
            def _():
                send(zs.at[j], zr.at[z], zr_s, zr_r, {"z": j})

    stages = (
        (0.0, relay), (2.0, raise_up), (3.1, across), (5.2, activate), (7.3, hand_over), (8.1, bring_down), (10.5, settle),
    )
    order = sorted((offset + turn, stage, turn) for stage, (offset, _) in enumerate(stages) for turn in range(4))
    pltpu.make_async_copy(wu_hbm, wu, in_sem.at[1]).wait()
    pltpu.make_async_copy(wdn_hbm, wdn, in_sem.at[2]).wait()
    for _, stage, turn in order:
        stages[stage][1](lax.rem(first + lean * PAIRS[turn] + 4, 4))
        if stage == 1 and turn == 0:
            squares()
        if stage == 2 and turn >= 2:
            renew(2 * turn, 2)

    zr[z] = zs[z]
    wait(sq2.at[pl.ds(0, 7)], sq2_r)
    wait(zr.at[pl.ds(0, 7)], zr_r)
    mean = jnp.sum(sq2[...], axis=0)[:, 0:1] / D
    squared = 1.0 / (mean + EPS)
    mlp = (jnp.sum(zr[...].astype(F32), axis=0) * squared).astype(BF16).astype(F32)
    out[...] = (res[z, rows, :].astype(F32) + mlp).astype(BF16)

    wait(hx.at[pl.ds(0, 3)], hx_s)
    wait(sq.at[pl.ds(0, 7)], sq_s)
    for number in range(14):
        wait(slot(0, 0), wo_s.at[number])
    for number, (home, array, columns) in enumerate(pieces):

        @pl.when(y != home)
        def _():
            wait(wb.at[0, :, columns], wb_s.at[number])

    for dx in range(NX):
        wait(half(hx, 0, 0), zb_s.at[2 * dx + 1])

        @pl.when(NC * around(x, dx, NX) + c != z)
        def _():
            wait(half(hx, 0, 0), zb_s.at[2 * dx])

    wait(xb.at[pl.ds(0, 28)], yb_s)

    by_width(lambda width: wait(pb.at[pl.ds(0, 19), :, slice(0, width)], rb_s))
    by_width(lambda width: wait(pb.at[pl.ds(0, 12), :, slice(0, width)], rl_s))

    wait(mb.at[pl.ds(0, 3)], mb_s)
    wait(hp.at[pl.ds(0, 3)], hp_s)
    wait(r2.at[pl.ds(0, 7)], op_s)
    wait(op.at[pl.ds(0, 7)], rz_s)
    wait(res.at[:, :, slice(0, 384)], ry_s)
    wait(sq2.at[pl.ds(0, 7)], sq2_s)
    wait(dd, dd_s)
    wait(us.at[pl.ds(0, 3)], us_s)
    wait(act.at[pl.ds(0, 7)], ac_s)
    wait(dyb.at[pl.ds(0, 3)], dy_s)
    wait(zr.at[pl.ds(0, 7)], zr_s)


def body(
    hidden_rows, carried_state, norm_gain, w_query, w_key, w_decay, w_value, w_gate,
    decay_bias, head_gain, w_out, mlp_gain, w_up, w_down,
):
    dma = pltpu.SemaphoreType.DMA
    vmem = pl.BlockSpec(memory_space=pltpu.VMEM)
    return pl.pallas_call(
        layer_kernel,
        out_shape=(pltpu.VMEM((16, 512), BF16), pltpu.VMEM((16, 65536), F32)),
        in_specs=[pl.BlockSpec(memory_space=pltpu.HBM)] * 14,
        out_specs=(vmem, vmem),
        scratch_shapes=[
            pltpu.VMEM((16, 512), BF16),
            pltpu.VMEM((4096,), BF16),
            pltpu.VMEM((256,), F32),
            pltpu.VMEM((256,), BF16),
            pltpu.VMEM((512,), BF16),
            pltpu.VMEM((NX, 16, 512), BF16),
            pltpu.VMEM((8, 16, 128), F32),
            pltpu.VMEM((32, 16, 512), BF16),
            pltpu.VMEM((NY, 128, 512), BF16),
            pltpu.VMEM((32, 16, 512), BF16),
            pltpu.VMEM((NY, 5, 16, 512), BF16),
            pltpu.VMEM((3, NY, 16, 512), BF16),
            pltpu.VMEM((16, 1792), F32),
            pltpu.VMEM((512, 1024), BF16),
            pltpu.VMEM((16, 65536), F32),
            pltpu.VMEM((16, 512), F32),
            pltpu.VMEM((16, 256), F32),
            pltpu.VMEM((16, 256), F32),
            pltpu.VMEM((512, 512), BF16),
            pltpu.VMEM((512, 512), BF16),
            pltpu.VMEM((NY, 16, 512), BF16),
            pltpu.VMEM((NY, 16, 128), BF16),
            pltpu.VMEM((8, 64, 128), BF16),
            pltpu.VMEM((8, 64, 128), BF16),
            pltpu.VMEM((NZ, 64, 512), BF16),
            pltpu.VMEM((8, 16, 128), F32),
            pltpu.VMEM((8, 64, 512), BF16),
            pltpu.VMEM((4, 64, 512), BF16),
            pltpu.VMEM((4, 64, 512), BF16),
            pltpu.VMEM((4, 64, 512), BF16),
            pltpu.VMEM((8, 64, 512), BF16),
            pltpu.VMEM((8, NY, 16, 512), BF16),
            pltpu.VMEM((NY, 8, 16, 512), BF16),
            pltpu.VMEM((8, 16, 512), BF16),
            pltpu.VMEM((NZ, 16, 512), BF16),
            dma((9,)), dma, dma((NX,)), dma, dma, dma((8,)), dma((NZ,)), dma, dma((32,)), dma((NZ,)),
            dma((5,)), dma, dma((14,)), dma((2, NZ)), dma, dma((NY,)), dma, dma((3,)),
            dma, dma, dma, dma, dma, dma, dma, dma((NZ,)), dma, dma((32,)), dma, dma,
            dma, dma((4,)), dma, dma((4,)), dma, dma((4,)), dma((4,)), dma, dma((4,)), dma, dma,
        ],
        compiler_params=pltpu.CompilerParams(collective_id=0, has_side_effects=True, vmem_limit_bytes=(59 << 20) + (800 << 10)),
        name="layer",
    )(
        hidden_rows, norm_gain, decay_bias, head_gain, mlp_gain, w_query, w_key, w_decay, w_value, w_gate,
        w_out, w_up, w_down, carried_state,
    )


def solution(mesh):
    finer = Mesh(mesh.devices.reshape(NZ, NY, NX, NC), ("z", "y", "x", "c"))
    placed = (
        P(KV, TP), P(KV, TP), P(), P(KV, TP), P(KV, TP), P(KV, TP), P(KV, TP), P(KV, TP),
        P(TP), P(), P(TP, KV), P(TP), P(TP, KV), P(KV, TP),
    )
    return jax.shard_map(
        body, mesh=finer, in_specs=placed, out_specs=(P(KV, TP), P(KV, TP)), check_vma=False
    )
```

```python
import jax
import jax.numpy as jnp
from jax import lax
from jax.experimental import pallas as pl
from jax.experimental.pallas import tpu as pltpu
from jax.sharding import Mesh
from jax.sharding import PartitionSpec as P

D = 4096
DK = 128
DV = 256
EPS = 1e-06
MESH = pl.DeviceIdType.MESH
F32 = jnp.float32
BF16 = jnp.bfloat16
KV = ("z", "y")
TP = ("x", "c")
NZ, NY, NX, NC = 8, 4, 4, 2
GROUPS = ((0, 1), (7, 2), (6, 3), (5, 4))
PAIRS = (0, 1, 3, 2)
KEYS = 32


def place():
    return tuple(lax.axis_index(name) for name in ("z", "y", "x", "c"))


def send(src, dst, sent, arrived, device):
    pltpu.make_async_remote_copy(
        src_ref=src, dst_ref=dst, send_sem=sent, recv_sem=arrived, device_id=device, device_id_type=MESH
    ).start()


def wait(ref, sem):
    pltpu.make_async_copy(ref, ref, sem).wait()


def greet(peers):
    for device in peers:
        pl.semaphore_signal(pltpu.get_barrier_semaphore(), inc=1, device_id=device, device_id_type=MESH)


def around(index, step, count):
    return lax.rem(index + step, count)


def layer_kernel(
    hid_hbm, norm_gain_hbm, bias_hbm, head_gain_hbm, mlp_gain_hbm,
    wq, wk, wd, wv, wg, wo, wu_hbm, wdn_hbm, state_hbm,
    out, new_state, hid, norm_gain, bias, head_gain, mlp_gain,
    hx, sq, xb, wb, pb, rb, rl, proj, wog, state, acc, decay, asked,
    wu, wdn, mb, hp, op, r2, res, sq2, upb, dd, us, ur, act, dp, dyb, zs, zr,
    in_sem, hx_s, hx_r, sq_s, sq_r, zb_s, zb_r, yb_s, yb_r, db_r, wb_s, wb_r, wo_s, wo_r, rb_s, rb_r, rl_s, rl_r,
    mb_s, mb_r, hp_s, hp_r, op_s, op_r, rz_s, rz_r, ry_s, ry_r, sq2_s, sq2_r,
    dd_s, dd_r, us_s, us_r, ac_s, ac_r, ad_r, dy_s, dy_r, zr_s, zr_r,
):
    z, y, x, c = place()
    kv = NY * z + y
    tp = NC * x + c
    small = (
        (hid_hbm, hid), (norm_gain_hbm, norm_gain), (bias_hbm, bias), (head_gain_hbm, head_gain), (mlp_gain_hbm, mlp_gain),
    )
    for number, (src, dst) in enumerate(small):
        pltpu.make_async_copy(src, dst, in_sem.at[4 + number]).start()
    pltpu.make_async_copy(state_hbm, state, in_sem.at[0]).start()
    pltpu.make_async_copy(wu_hbm, wu, in_sem.at[1]).start()
    pltpu.make_async_copy(wdn_hbm, wdn, in_sem.at[2]).start()
    tps = [
        {"x": around(x, dx, NX), "c": around(c, dc, NC)} for dx in (2, 1, 3, 0) for dc in range(NC) if dx or dc
    ]
    ys = [{"y": around(y, dy, NY)} for dy in (2, 1, 3)]
    zfar = [{"z": around(z, dz, NZ)} for dz in (4, 3, 5, 2, 6, 1, 7)]
    peers = tps + zfar + [{"z": device["z"], "c": 1 - c} for device in zfar] + ys
    greet(peers)
    for number, (src, dst) in enumerate(small):
        pltpu.make_async_copy(src, dst, in_sem.at[4 + number]).wait()
    h = hid[...].astype(F32)
    gain = norm_gain[pl.ds(pl.multiple_of(tp * 512, 512), 512)].astype(F32).reshape(1, 512)
    hx[x] = (h * gain).astype(BF16)
    sq[tp] = jnp.broadcast_to(jnp.sum(h * h, axis=-1, keepdims=True), (16, 128))
    pl.semaphore_wait(pltpu.get_barrier_semaphore(), len(peers))

    def lanes(index, width):
        return pl.ds(pl.multiple_of(index * width, width), width)

    side = 1 - 2 * c

    def at(offset):
        return lax.rem(z + offset * side + NZ, NZ)

    def slot(origin, part):
        return wog.at[pl.ds(part * 256, 256), lanes(origin, 128)]

    for dx in (2, 1, 3):
        send(hx.at[x], hx.at[x], hx_s, hx_r.at[x], {"x": around(x, dx, NX)})
    for device in tps:
        send(sq.at[tp], sq.at[tp], sq_s, sq_r, device)
    up, down = around(z, 1, NZ), around(z, NZ - 1, NZ)
    for part in range(2):
        mine = wo.at[pl.ds(part * 256, 256)]
        send(mine, slot(z, part), wo_s.at[7 * part], wo_r.at[part, z], {"z": up})
        send(mine, slot(z, part), wo_s.at[7 * part + 1], wo_r.at[part, z], {"z": down})
    own_out = pltpu.make_async_copy(wo, wog.at[:, lanes(z, 128)], in_sem.at[3])
    own_out.start()
    pieces = (
        (0, wv, slice(0, 512)),
        (1, wg, slice(0, 512)),
        (2, wq, slice(0, 256)),
        (2, wk, slice(256, 512)),
        (3, wd, slice(0, 256)),
    )
    for number, (home, array, columns) in enumerate(pieces):
        target = wb.at[y, :, columns]

        @pl.when(y != home)
        def _():
            send(array, target, wb_s.at[number], wb_r, {"y": home})

        @pl.when(y == home)
        def _():
            pltpu.make_async_copy(array, target, wb_r).start()

    for dy in (2, 1, 3):
        yt = around(y, dy, NY)
        send(hid.at[:, lanes(yt, 128)], hp.at[y], hp_s, hp_r, {"y": yt})
    hp[y] = hid[:, lanes(y, 128)]

    def pass_on(step, part):
        low = around(z, NZ - step + 1, NZ)
        wait(slot(low, part), wo_r.at[part, low])
        send(slot(low, part), slot(low, part), wo_s.at[7 * part + 2 * step - 2], wo_r.at[part, low], {"z": up})
        high = around(z, step - 1, NZ)
        wait(slot(high, part), wo_r.at[part, high])
        if step < 4:
            send(slot(high, part), slot(high, part), wo_s.at[7 * part + 2 * step - 1], wo_r.at[part, high], {"z": down})

    def half(ref, number, which):
        return ref.at[number, :, lanes(which, 256)]

    for dx in (0, 1, 3, 2):
        xs = around(x, dx, NX)
        if dx:
            wait(hx.at[xs], hx_r.at[xs])
        zt = NC * xs + c
        for dc in range(NC):
            core = around(c, dc, NC)
            src, dst = half(hx, xs, core), half(xb, kv, core)
            if dc:
                send(src, dst, zb_s.at[2 * dx + dc], zb_r.at[z], {"z": zt, "c": core})
            else:

                @pl.when(zt != z)
                def _():
                    send(src, dst, zb_s.at[2 * dx], zb_r.at[z], {"z": zt, "c": core})

                @pl.when(zt == z)
                def _():
                    pltpu.make_async_copy(src, dst, zb_r.at[z]).start()

    def spread_y(group):
        for dz in group:
            zt = at(dz)
            number = NY * zt + y
            piece = half(xb, number, c)
            wait(piece, zb_r.at[zt])
            for device in ys:
                send(piece, piece, yb_s, yb_r.at[number], device)
            send(piece, piece, yb_s, db_r.at[zt], {"c": 1 - c})

    def spread_c(group):
        for dz in group:
            zt = at(dz)
            for dy in (1, 3, 2):
                number = NY * zt + around(y, dy, NY)
                piece = half(xb, number, c)
                wait(piece, yb_r.at[number])
                send(piece, piece, yb_s, db_r.at[zt], {"c": 1 - c})

    def plane(offset):
        return pl.ds(pl.multiple_of(NY * at(offset), NY), NY)

    def by_width(action):
        @pl.when(y < 3)
        def _():
            action(512)

        @pl.when(y == 3)
        def _():
            action(256)

    def scatter(offset, kind, width):
        for dy in (2, 1, 3, 0):
            yt = around(y, dy, NY)
            src = pb.at[NY * at(offset) + yt, :, slice(0, width)]
            dst = rb.at[y, kind, :, slice(0, width)]
            if offset or dy:
                send(src, dst, rb_s, rb_r.at[y], {"z": at(offset), "y": yt})
            else:
                pltpu.make_async_copy(src, dst, rb_r.at[y]).start()

    def lend(offset, number, via, width):
        src, dst = pb.at[plane(offset), :, slice(0, width)], rl.at[number, :, :, slice(0, width)]
        send(src, dst, rl_s, rl_r.at[number], {"z": at(via)})

    def combine(offset, number, kind, width):
        wait(rl.at[number, :, :, slice(0, width)], rl_r.at[number])
        total = pb[plane(offset), :, 0:width].astype(F32) + rl[number, :, :, 0:width].astype(F32)
        pb[plane(offset), :, 0:width] = total.astype(BF16)
        scatter(offset, kind, width)

    def multiply(group):
        for dz in group:
            wait(xb.at[plane(dz), :, slice(0, 256)], db_r.at[at(dz)])
        rows = [xb[plane(dz)].reshape(64, 512) for dz in group]
        weights = wb[...].reshape(512, 512)
        part = jnp.dot(jnp.concatenate(rows, axis=0), weights, preferred_element_type=F32).astype(BF16)
        for number, dz in enumerate(group):
            pb[plane(dz)] = part[64 * number : 64 * number + 64].reshape(NY, 16, 512)

    spread_y(GROUPS[0])
    pass_on(2, 0)
    spread_y(GROUPS[1])
    pass_on(2, 1)
    spread_y(GROUPS[2])
    spread_y(GROUPS[3])
    spread_c(GROUPS[0])
    pass_on(3, 0)
    spread_c(GROUPS[1])
    pass_on(3, 1)
    by_width(lambda width: wait(wb.at[:, :, slice(0, width)], wb_r))
    multiply(GROUPS[0])
    spread_c(GROUPS[2])
    by_width(lambda width: scatter(0, 0, width))
    multiply(GROUPS[1])
    spread_c(GROUPS[3])
    by_width(lambda width: (lend(2, 0, 1, width), scatter(7, 4, width)))
    multiply(GROUPS[3])
    by_width(lambda width: (lend(4, 1, 1, width), lend(5, 2, 7, width)))
    multiply(GROUPS[2])
    by_width(lambda width: combine(1, 0, 1, width))
    pass_on(4, 0)
    by_width(lambda width: combine(3, 1, 2, width))
    by_width(lambda width: combine(6, 2, 3, width))
    pass_on(4, 1)

    wait(sq.at[pl.ds(0, 7)], sq_r)
    scale = lax.rsqrt(jnp.sum(sq[...], axis=0) / D + EPS)[:, 0:1]

    def summed(block, width, offset):
        wait(rb.at[block, :, :, slice(0, width)], rb_r.at[block])
        total = jnp.sum(rb[block, :, :, 0:width].astype(F32), axis=0)
        proj[:, offset : offset + width] = (total * scale).astype(BF16).astype(F32)

    summed(3, 256, 0)
    summed(2, 512, 256)
    summed(0, 512, 768)
    summed(1, 512, 1280)
    pre = proj[:, 0:256] + bias[...].reshape(1, 256)
    soft = jnp.minimum(pre, 0.0) - jnp.log1p(jnp.exp(-jnp.abs(pre)))
    decay[...] = jnp.exp(soft / 16.0)
    acc[...] = jnp.zeros_like(acc)
    queries, keys_now = proj[:, 256:512] * DK ** (-0.5), proj[:, 512:768]
    asked[...] = queries * decay[...]
    for head in range(2):
        columns = slice(head * DK, head * DK + DK)
        meet = jnp.sum(queries[:, columns] * keys_now[:, columns], axis=-1, keepdims=True)
        acc[:, head * DV : head * DV + DV] = meet * proj[:, 768 + head * DV : 768 + head * DV + DV]
    pltpu.make_async_copy(state_hbm, state, in_sem.at[0]).wait()

    def turned(ref, step):
        return pltpu.roll(ref, lax.rem(256 - step * KEYS, 256), axis=1)

    for head in range(2):
        columns = slice(head * DV, head * DV + DV)
        totals = [acc[:, columns]] + [jnp.zeros((16, DV), F32)] * 3
        for key in range(head * DK, head * DK + DK):
            weight = asked[:, key : key + 1]
            totals[key % 4] = totals[key % 4] + weight * state[:, key * DV : key * DV + DV]
        acc[:, columns] = (totals[0] + totals[1]) + (totals[2] + totals[3])

    def renew(first_step, steps):
        @pl.loop(first_step, first_step + steps)
        def _(step):
            rates = turned(decay[...], step)
            keys = turned(proj[:, 512:768], step)
            values = proj[:, pl.ds(pl.multiple_of(768 + step // (DK // KEYS) * DV, DV), DV)]
            for key in range(KEYS):
                where = pl.ds(pl.multiple_of((step * KEYS + key) * DV, DV), DV)
                new_state[:, where] = rates[:, key : key + 1] * state[:, where] + keys[:, key : key + 1] * values

    for number in range(2):
        part = slice(number * DV, number * DV + DV)
        value = acc[:, part]
        gate = proj[:, 1280 + number * DV : 1280 + number * DV + DV]
        normal = value * lax.rsqrt(jnp.mean(value * value, axis=-1, keepdims=True) + EPS)
        silu = gate / (1.0 + jnp.exp(-gate))
        mb[y, :, part] = (normal * head_gain[...].astype(F32).reshape(1, DV) * silu).astype(BF16)
    for device in ys:
        send(mb.at[y], mb.at[y], mb_s, mb_r, device)
    renew(0, 4)
    here = lanes(y, 128)
    last = around(z, 4, NZ)
    for part in range(2):
        wait(slot(last, part), wo_r.at[part, last])
    own_out.wait()
    wait(mb.at[pl.ds(0, 3)], mb_r)
    part = jnp.dot(mb[...].reshape(64, 512), wog[...], preferred_element_type=F32).astype(BF16)
    for t in range(8):
        op[t] = part[:, t * 128 : t * 128 + 128]
    r2[tp] = op[tp]
    for device in tps:
        t = NC * device["x"] + device["c"]
        send(op.at[t], r2.at[tp], op_s, op_r, device)
    renew(4, 4)
    wait(hp.at[pl.ds(0, 3)], hp_r)
    wait(r2.at[pl.ds(0, 7)], op_r)
    attn = jnp.sum(r2[...].astype(F32), axis=0).astype(BF16).astype(F32)
    res[z, :, here] = (hp[...].reshape(64, 128).astype(F32) + attn).astype(BF16)
    mine = res.at[z, :, here]
    first = z // 2
    lean = 2 * (z % 2) - 1
    pairs = [lax.rem(first + lean * turn + 4, 4) for turn in PAIRS]
    for zt in [z - lean] + [2 * pair + k for pair in pairs[1:] for k in range(2)]:
        send(mine, mine, rz_s, rz_r.at[z], {"z": zt})
    for device in ys:
        send(mine, mine, ry_s, ry_r.at[kv], device)

    rows = pl.ds(pl.multiple_of(y * 16, 16), 16)

    def two(pair):
        return pl.ds(pl.multiple_of(2 * pair, 2), 2)

    def relay(pair):
        for k in range(2):
            zt = 2 * pair + k
            piece = res.at[zt, :, here]

            @pl.when(zt != z)
            def _():
                wait(piece, rz_r.at[zt])
                for device in ys:
                    send(piece, piece, ry_s, ry_r.at[NY * zt + y], device)

    def raise_up(pair):
        for k in range(2):
            zt = 2 * pair + k
            for dy in (1, 3, 2):
                yt = around(y, dy, NY)
                wait(res.at[zt, :, lanes(yt, 128)], ry_r.at[NY * zt + yt])
        both = res[two(pair)].reshape(128, 512).astype(F32)
        fed = (both * mlp_gain[...].astype(F32).reshape(1, 512)).astype(BF16)
        part = jnp.dot(fed, wu[...], preferred_element_type=F32).astype(BF16)
        upb[two(pair)] = part.reshape(2, 64, 512)
        send(upb.at[2 * pair + 1 - c], dd.at[pair], dd_s, dd_r.at[pair], {"c": 1 - c})

    def squares():
        own = res[z, rows, :].astype(F32)
        sq2[tp] = jnp.broadcast_to(jnp.sum(own * own, axis=-1, keepdims=True), (16, 128))
        for device in tps:
            send(sq2.at[tp], sq2.at[tp], sq2_s, sq2_r, device)

    def across(pair):
        wait(dd.at[pair], dd_r.at[pair])
        total = upb[2 * pair + c].astype(F32) + dd[pair].astype(F32)
        us[pair] = total.astype(BF16).reshape(NX, 16, 512)
        for dx in (2, 1, 3):
            xs = around(x, dx, NX)
            send(us.at[pair, xs], ur.at[pair, x], us_s, us_r.at[pair], {"x": xs})

    def activate(pair):
        wait(ur.at[pair, pl.ds(0, 3)], us_r.at[pair])
        total = us[pair, x].astype(F32)
        for dx in (1, 3, 2):
            total = total + ur[pair, around(x, dx, NX)].astype(F32)
        act[2 * pair + c, x] = jnp.square(jnp.maximum(total, 0.0)).astype(BF16)
        piece = act.at[2 * pair + c, x]
        for dx in (2, 1, 3):
            send(piece, piece, ac_s, ac_r.at[pair], {"x": around(x, dx, NX)})

    def hand_over(pair):
        piece = act.at[2 * pair + c]
        wait(piece.at[pl.ds(0, 3)], ac_r.at[pair])
        send(piece, piece, ac_s, ad_r.at[pair], {"c": 1 - c})

    def bring_down(pair):
        wait(act.at[NC * pair + 1 - c], ad_r.at[pair])
        part = jnp.dot(act[two(pair)].reshape(128, 512), wdn[...], preferred_element_type=F32).astype(BF16)
        dp[two(pair)] = part.reshape(2, NY, 16, 512)
        for device in ys:
            send(dp.at[two(pair), device["y"]], dyb.at[y, two(pair)], dy_s, dy_r.at[pair], device)

    def settle(pair):
        wait(dyb.at[pl.ds(0, 3), two(pair)], dy_r.at[pair])
        total = dp[two(pair), y].astype(F32)
        for dy in (1, 2, 3):
            total = total + dyb[around(y, dy, NY), two(pair)].astype(F32)
        zs[two(pair)] = total.astype(BF16)
        for k in range(2):
            j = 2 * pair + k

            @pl.when(j != z)
            def _():
                send(zs.at[j], zr.at[z], zr_s, zr_r, {"z": j})

    stages = (
        (0.0, relay), (2.0, raise_up), (3.1, across), (5.2, activate), (7.3, hand_over), (8.4, bring_down), (10.5, settle),
    )
    order = sorted((offset + turn, stage, turn) for stage, (offset, _) in enumerate(stages) for turn in range(4))
    pltpu.make_async_copy(wu_hbm, wu, in_sem.at[1]).wait()
    pltpu.make_async_copy(wdn_hbm, wdn, in_sem.at[2]).wait()
    for _, stage, turn in order:
        stages[stage][1](pairs[turn])
        if stage == 1 and turn == 0:
            squares()

    zr[z] = zs[z]
    wait(sq2.at[pl.ds(0, 7)], sq2_r)
    wait(zr.at[pl.ds(0, 7)], zr_r)
    mean = jnp.sum(sq2[...], axis=0)[:, 0:1] / D
    squared = 1.0 / (mean + EPS)
    mlp = (jnp.sum(zr[...].astype(F32), axis=0) * squared).astype(BF16).astype(F32)
    out[...] = (res[z, rows, :].astype(F32) + mlp).astype(BF16)

    wait(hx.at[pl.ds(0, 3)], hx_s)
    wait(sq.at[pl.ds(0, 7)], sq_s)
    for number in range(14):
        wait(slot(0, 0), wo_s.at[number])
    for number, (home, array, columns) in enumerate(pieces):

        @pl.when(y != home)
        def _():
            wait(wb.at[0, :, columns], wb_s.at[number])

    for dx in range(NX):
        wait(half(hx, 0, 0), zb_s.at[2 * dx + 1])

        @pl.when(NC * around(x, dx, NX) + c != z)
        def _():
            wait(half(hx, 0, 0), zb_s.at[2 * dx])

    wait(xb.at[pl.ds(0, 28)], yb_s)

    by_width(lambda width: wait(pb.at[pl.ds(0, 19), :, slice(0, width)], rb_s))
    by_width(lambda width: wait(pb.at[pl.ds(0, 12), :, slice(0, width)], rl_s))

    wait(mb.at[pl.ds(0, 3)], mb_s)
    wait(hp.at[pl.ds(0, 3)], hp_s)
    wait(r2.at[pl.ds(0, 7)], op_s)
    wait(op.at[pl.ds(0, 7)], rz_s)
    wait(res.at[:, :, slice(0, 384)], ry_s)
    wait(sq2.at[pl.ds(0, 7)], sq2_s)
    wait(dd, dd_s)
    wait(us.at[pl.ds(0, 3)], us_s)
    wait(act.at[pl.ds(0, 7)], ac_s)
    wait(dyb.at[pl.ds(0, 3)], dy_s)
    wait(zr.at[pl.ds(0, 7)], zr_s)


def body(
    hidden_rows, carried_state, norm_gain, w_query, w_key, w_decay, w_value, w_gate,
    decay_bias, head_gain, w_out, mlp_gain, w_up, w_down,
):
    dma = pltpu.SemaphoreType.DMA
    vmem = pl.BlockSpec(memory_space=pltpu.VMEM)
    return pl.pallas_call(
        layer_kernel,
        out_shape=(pltpu.VMEM((16, 512), BF16), pltpu.VMEM((16, 65536), F32)),
        in_specs=[pl.BlockSpec(memory_space=pltpu.HBM)] * 14,
        out_specs=(vmem, vmem),
        scratch_shapes=[
            pltpu.VMEM((16, 512), BF16),
            pltpu.VMEM((4096,), BF16),
            pltpu.VMEM((256,), F32),
            pltpu.VMEM((256,), BF16),
            pltpu.VMEM((512,), BF16),
            pltpu.VMEM((NX, 16, 512), BF16),
            pltpu.VMEM((8, 16, 128), F32),
            pltpu.VMEM((32, 16, 512), BF16),
            pltpu.VMEM((NY, 128, 512), BF16),
            pltpu.VMEM((32, 16, 512), BF16),
            pltpu.VMEM((NY, 5, 16, 512), BF16),
            pltpu.VMEM((3, NY, 16, 512), BF16),
            pltpu.VMEM((16, 1792), F32),
            pltpu.VMEM((512, 1024), BF16),
            pltpu.VMEM((16, 65536), F32),
            pltpu.VMEM((16, 512), F32),
            pltpu.VMEM((16, 256), F32),
            pltpu.VMEM((16, 256), F32),
            pltpu.VMEM((512, 512), BF16),
            pltpu.VMEM((512, 512), BF16),
            pltpu.VMEM((NY, 16, 512), BF16),
            pltpu.VMEM((NY, 16, 128), BF16),
            pltpu.VMEM((8, 64, 128), BF16),
            pltpu.VMEM((8, 64, 128), BF16),
            pltpu.VMEM((NZ, 64, 512), BF16),
            pltpu.VMEM((8, 16, 128), F32),
            pltpu.VMEM((8, 64, 512), BF16),
            pltpu.VMEM((4, 64, 512), BF16),
            pltpu.VMEM((4, NX, 16, 512), BF16),
            pltpu.VMEM((4, NX, 16, 512), BF16),
            pltpu.VMEM((8, NX, 16, 512), BF16),
            pltpu.VMEM((8, NY, 16, 512), BF16),
            pltpu.VMEM((NY, 8, 16, 512), BF16),
            pltpu.VMEM((8, 16, 512), BF16),
            pltpu.VMEM((NZ, 16, 512), BF16),
            dma((9,)), dma, dma((NX,)), dma, dma, dma((8,)), dma((NZ,)), dma, dma((32,)), dma((NZ,)),
            dma((5,)), dma, dma((14,)), dma((2, NZ)), dma, dma((NY,)), dma, dma((3,)),
            dma, dma, dma, dma, dma, dma, dma, dma((NZ,)), dma, dma((32,)), dma, dma,
            dma, dma((4,)), dma, dma((4,)), dma, dma((4,)), dma((4,)), dma, dma((4,)), dma, dma,
        ],
        compiler_params=pltpu.CompilerParams(collective_id=0, has_side_effects=True, vmem_limit_bytes=(59 << 20) + (800 << 10)),
        name="layer",
    )(
        hidden_rows, norm_gain, decay_bias, head_gain, mlp_gain, w_query, w_key, w_decay, w_value, w_gate,
        w_out, w_up, w_down, carried_state,
    )


def solution(mesh):
    finer = Mesh(mesh.devices.reshape(NZ, NY, NX, NC), ("z", "y", "x", "c"))
    placed = (
        P(KV, TP), P(KV, TP), P(), P(KV, TP), P(KV, TP), P(KV, TP), P(KV, TP), P(KV, TP),
        P(TP), P(), P(TP, KV), P(TP), P(TP, KV), P(KV, TP),
    )
    return jax.shard_map(
        body, mesh=finer, in_specs=placed, out_specs=(P(KV, TP), P(KV, TP)), check_vma=False
    )
```

```python
import jax
import jax.numpy as jnp
from jax import lax
from jax.experimental import pallas as pl
from jax.experimental.pallas import tpu as pltpu
from jax.sharding import Mesh
from jax.sharding import PartitionSpec as P

D = 4096
DK = 128
DV = 256
EPS = 1e-06
MESH = pl.DeviceIdType.MESH
F32 = jnp.float32
BF16 = jnp.bfloat16
KV = ("z", "y")
TP = ("x", "c")
NZ, NY, NX, NC = 8, 4, 4, 2
GROUPS = ((0, 1), (7, 2), (6, 3), (5, 4))
PAIRS = (0, 1, 2, 3)
KEYS = 32


def place():
    return tuple(lax.axis_index(name) for name in ("z", "y", "x", "c"))


def send(src, dst, sent, arrived, device):
    pltpu.make_async_remote_copy(
        src_ref=src, dst_ref=dst, send_sem=sent, recv_sem=arrived, device_id=device, device_id_type=MESH
    ).start()


def wait(ref, sem):
    pltpu.make_async_copy(ref, ref, sem).wait()


def greet(peers):
    for device in peers:
        pl.semaphore_signal(pltpu.get_barrier_semaphore(), inc=1, device_id=device, device_id_type=MESH)


def around(index, step, count):
    return lax.rem(index + step, count)


def layer_kernel(
    hid_hbm, norm_gain_hbm, bias_hbm, head_gain_hbm, mlp_gain_hbm,
    wq, wk, wd, wv, wg, wo, wu_hbm, wdn_hbm, state_hbm,
    out, new_state, hid, norm_gain, bias, head_gain, mlp_gain,
    hx, sq, xb, wb, pb, rb, rl, proj, wog, state, acc, decay, asked,
    wu, wdn, mb, hp, op, r2, res, sq2, upb, dd, us, ur, act, dp, dyb, zs, zr,
    in_sem, hx_s, hx_r, sq_s, sq_r, zb_s, zb_r, yb_s, yb_r, db_r, wb_s, wb_r, wo_s, wo_r, rb_s, rb_r, rl_s, rl_r,
    mb_s, mb_r, hp_s, hp_r, op_s, op_r, rz_s, rz_r, ry_s, ry_r, sq2_s, sq2_r,
    dd_s, dd_r, us_s, us_r, ac_s, ac_r, ad_r, dy_s, dy_r, zr_s, zr_r,
):
    z, y, x, c = place()
    kv = NY * z + y
    tp = NC * x + c
    small = (
        (hid_hbm, hid), (norm_gain_hbm, norm_gain), (bias_hbm, bias), (head_gain_hbm, head_gain), (mlp_gain_hbm, mlp_gain),
    )
    for number, (src, dst) in enumerate(small):
        pltpu.make_async_copy(src, dst, in_sem.at[4 + number]).start()
    pltpu.make_async_copy(state_hbm, state, in_sem.at[0]).start()
    pltpu.make_async_copy(wu_hbm, wu, in_sem.at[1]).start()
    pltpu.make_async_copy(wdn_hbm, wdn, in_sem.at[2]).start()
    tps = [
        {"x": around(x, dx, NX), "c": around(c, dc, NC)} for dx in (2, 1, 3, 0) for dc in range(NC) if dx or dc
    ]
    ys = [{"y": around(y, dy, NY)} for dy in (2, 1, 3)]
    zfar = [{"z": around(z, dz, NZ)} for dz in (4, 3, 5, 2, 6, 1, 7)]
    peers = tps + zfar + [{"z": device["z"], "c": 1 - c} for device in zfar] + ys
    greet(peers)
    for number, (src, dst) in enumerate(small):
        pltpu.make_async_copy(src, dst, in_sem.at[4 + number]).wait()
    h = hid[...].astype(F32)
    gain = norm_gain[pl.ds(pl.multiple_of(tp * 512, 512), 512)].astype(F32).reshape(1, 512)
    hx[x] = (h * gain).astype(BF16)
    sq[tp] = jnp.broadcast_to(jnp.sum(h * h, axis=-1, keepdims=True), (16, 128))
    pl.semaphore_wait(pltpu.get_barrier_semaphore(), len(peers))

    def lanes(index, width):
        return pl.ds(pl.multiple_of(index * width, width), width)

    side = 1 - 2 * c

    def at(offset):
        return lax.rem(z + offset * side + NZ, NZ)

    def slot(origin, part):
        return wog.at[pl.ds(part * 256, 256), lanes(origin, 128)]

    for dx in (2, 1, 3):
        send(hx.at[x], hx.at[x], hx_s, hx_r.at[x], {"x": around(x, dx, NX)})
    for device in tps:
        send(sq.at[tp], sq.at[tp], sq_s, sq_r, device)
    up, down = around(z, 1, NZ), around(z, NZ - 1, NZ)
    for part in range(2):
        mine = wo.at[pl.ds(part * 256, 256)]
        send(mine, slot(z, part), wo_s.at[7 * part], wo_r.at[part, z], {"z": up})
        send(mine, slot(z, part), wo_s.at[7 * part + 1], wo_r.at[part, z], {"z": down})
    own_out = pltpu.make_async_copy(wo, wog.at[:, lanes(z, 128)], in_sem.at[3])
    own_out.start()
    pieces = (
        (0, wv, slice(0, 512)),
        (1, wg, slice(0, 512)),
        (2, wq, slice(0, 256)),
        (2, wk, slice(256, 512)),
        (3, wd, slice(0, 256)),
    )
    for number, (home, array, columns) in enumerate(pieces):
        target = wb.at[y, :, columns]

        @pl.when(y != home)
        def _():
            send(array, target, wb_s.at[number], wb_r, {"y": home})

        @pl.when(y == home)
        def _():
            pltpu.make_async_copy(array, target, wb_r).start()

    for dy in (2, 1, 3):
        yt = around(y, dy, NY)
        send(hid.at[:, lanes(yt, 128)], hp.at[y], hp_s, hp_r, {"y": yt})
    hp[y] = hid[:, lanes(y, 128)]

    def pass_on(step, part):
        low = around(z, NZ - step + 1, NZ)
        wait(slot(low, part), wo_r.at[part, low])
        send(slot(low, part), slot(low, part), wo_s.at[7 * part + 2 * step - 2], wo_r.at[part, low], {"z": up})
        high = around(z, step - 1, NZ)
        wait(slot(high, part), wo_r.at[part, high])
        if step < 4:
            send(slot(high, part), slot(high, part), wo_s.at[7 * part + 2 * step - 1], wo_r.at[part, high], {"z": down})

    def half(ref, number, which):
        return ref.at[number, :, lanes(which, 256)]

    for dx in (0, 1, 3, 2):
        xs = around(x, dx, NX)
        if dx:
            wait(hx.at[xs], hx_r.at[xs])
        zt = NC * xs + c
        for dc in range(NC):
            core = around(c, dc, NC)
            src, dst = half(hx, xs, core), half(xb, kv, core)
            if dc:
                send(src, dst, zb_s.at[2 * dx + dc], zb_r.at[z], {"z": zt, "c": core})
            else:

                @pl.when(zt != z)
                def _():
                    send(src, dst, zb_s.at[2 * dx], zb_r.at[z], {"z": zt, "c": core})

                @pl.when(zt == z)
                def _():
                    pltpu.make_async_copy(src, dst, zb_r.at[z]).start()

    def spread_y(group):
        for dz in group:
            zt = at(dz)
            number = NY * zt + y
            piece = half(xb, number, c)
            wait(piece, zb_r.at[zt])
            for device in ys:
                send(piece, piece, yb_s, yb_r.at[number], device)
            send(piece, piece, yb_s, db_r.at[zt], {"c": 1 - c})

    def spread_c(group):
        for dz in group:
            zt = at(dz)
            for dy in (1, 3, 2):
                number = NY * zt + around(y, dy, NY)
                piece = half(xb, number, c)
                wait(piece, yb_r.at[number])
                send(piece, piece, yb_s, db_r.at[zt], {"c": 1 - c})

    def plane(offset):
        return pl.ds(pl.multiple_of(NY * at(offset), NY), NY)

    def by_width(action):
        @pl.when(y < 3)
        def _():
            action(512)

        @pl.when(y == 3)
        def _():
            action(256)

    def scatter(offset, kind, width):
        for dy in (2, 1, 3, 0):
            yt = around(y, dy, NY)
            src = pb.at[NY * at(offset) + yt, :, slice(0, width)]
            dst = rb.at[y, kind, :, slice(0, width)]
            if offset or dy:
                send(src, dst, rb_s, rb_r.at[y], {"z": at(offset), "y": yt})
            else:
                pltpu.make_async_copy(src, dst, rb_r.at[y]).start()

    def lend(offset, number, via, width):
        src, dst = pb.at[plane(offset), :, slice(0, width)], rl.at[number, :, :, slice(0, width)]
        send(src, dst, rl_s, rl_r.at[number], {"z": at(via)})

    def combine(offset, number, kind, width):
        wait(rl.at[number, :, :, slice(0, width)], rl_r.at[number])
        total = pb[plane(offset), :, 0:width].astype(F32) + rl[number, :, :, 0:width].astype(F32)
        pb[plane(offset), :, 0:width] = total.astype(BF16)
        scatter(offset, kind, width)

    def multiply(group):
        for dz in group:
            wait(xb.at[plane(dz), :, slice(0, 256)], db_r.at[at(dz)])
        rows = [xb[plane(dz)].reshape(64, 512) for dz in group]
        weights = wb[...].reshape(512, 512)
        part = jnp.dot(jnp.concatenate(rows, axis=0), weights, preferred_element_type=F32).astype(BF16)
        for number, dz in enumerate(group):
            pb[plane(dz)] = part[64 * number : 64 * number + 64].reshape(NY, 16, 512)

    spread_y(GROUPS[0])
    pass_on(2, 0)
    spread_y(GROUPS[1])
    pass_on(2, 1)
    spread_y(GROUPS[2])
    spread_y(GROUPS[3])
    spread_c(GROUPS[0])
    pass_on(3, 0)
    spread_c(GROUPS[1])
    pass_on(3, 1)
    by_width(lambda width: wait(wb.at[:, :, slice(0, width)], wb_r))
    multiply(GROUPS[0])
    spread_c(GROUPS[2])
    by_width(lambda width: scatter(0, 0, width))
    multiply(GROUPS[1])
    spread_c(GROUPS[3])
    by_width(lambda width: lend(2, 0, 1, width))
    multiply(GROUPS[3])
    by_width(lambda width: (lend(4, 1, 1, width), lend(5, 2, 7, width), scatter(7, 4, width)))
    multiply(GROUPS[2])
    by_width(lambda width: combine(1, 0, 1, width))
    by_width(lambda width: combine(3, 1, 2, width))
    by_width(lambda width: combine(6, 2, 3, width))
    pass_on(4, 0)
    pass_on(4, 1)

    wait(sq.at[pl.ds(0, 7)], sq_r)
    scale = lax.rsqrt(jnp.sum(sq[...], axis=0) / D + EPS)[:, 0:1]

    def summed(block, width, offset):
        wait(rb.at[block, :, :, slice(0, width)], rb_r.at[block])
        total = jnp.sum(rb[block, :, :, 0:width].astype(F32), axis=0)
        proj[:, offset : offset + width] = (total * scale).astype(BF16).astype(F32)

    summed(3, 256, 0)
    summed(2, 512, 256)
    summed(0, 512, 768)
    summed(1, 512, 1280)
    pre = proj[:, 0:256] + bias[...].reshape(1, 256)
    soft = jnp.minimum(pre, 0.0) - jnp.log1p(jnp.exp(-jnp.abs(pre)))
    decay[...] = jnp.exp(soft / 16.0)
    acc[...] = jnp.zeros_like(acc)
    queries, keys_now = proj[:, 256:512] * DK ** (-0.5), proj[:, 512:768]
    asked[...] = queries * decay[...]
    for head in range(2):
        columns = slice(head * DK, head * DK + DK)
        meet = jnp.sum(queries[:, columns] * keys_now[:, columns], axis=-1, keepdims=True)
        acc[:, head * DV : head * DV + DV] = meet * proj[:, 768 + head * DV : 768 + head * DV + DV]
    pltpu.make_async_copy(state_hbm, state, in_sem.at[0]).wait()

    def turned(ref, step):
        return pltpu.roll(ref, lax.rem(256 - step * KEYS, 256), axis=1)

    for head in range(2):
        columns = slice(head * DV, head * DV + DV)
        totals = [acc[:, columns]] + [jnp.zeros((16, DV), F32)] * 3
        for key in range(head * DK, head * DK + DK):
            weight = asked[:, key : key + 1]
            totals[key % 4] = totals[key % 4] + weight * state[:, key * DV : key * DV + DV]
        acc[:, columns] = (totals[0] + totals[1]) + (totals[2] + totals[3])

    def renew(first_step, steps):
        @pl.loop(first_step, first_step + steps)
        def _(step):
            rates = turned(decay[...], step)
            keys = turned(proj[:, 512:768], step)
            values = proj[:, pl.ds(pl.multiple_of(768 + step // (DK // KEYS) * DV, DV), DV)]
            for key in range(KEYS):
                where = pl.ds(pl.multiple_of((step * KEYS + key) * DV, DV), DV)
                new_state[:, where] = rates[:, key : key + 1] * state[:, where] + keys[:, key : key + 1] * values

    for number in range(2):
        part = slice(number * DV, number * DV + DV)
        value = acc[:, part]
        gate = proj[:, 1280 + number * DV : 1280 + number * DV + DV]
        normal = value * lax.rsqrt(jnp.mean(value * value, axis=-1, keepdims=True) + EPS)
        silu = gate / (1.0 + jnp.exp(-gate))
        mb[y, :, part] = (normal * head_gain[...].astype(F32).reshape(1, DV) * silu).astype(BF16)
    for device in ys:
        send(mb.at[y], mb.at[y], mb_s, mb_r, device)
    here = lanes(y, 128)
    last = around(z, 4, NZ)
    for part in range(2):
        wait(slot(last, part), wo_r.at[part, last])
    own_out.wait()
    wait(mb.at[pl.ds(0, 3)], mb_r)
    part = jnp.dot(mb[...].reshape(64, 512), wog[...], preferred_element_type=F32).astype(BF16)
    for t in range(8):
        op[t] = part[:, t * 128 : t * 128 + 128]
    r2[tp] = op[tp]
    for device in tps:
        t = NC * device["x"] + device["c"]
        send(op.at[t], r2.at[tp], op_s, op_r, device)
    wait(hp.at[pl.ds(0, 3)], hp_r)
    wait(r2.at[pl.ds(0, 7)], op_r)
    attn = jnp.sum(r2[...].astype(F32), axis=0).astype(BF16).astype(F32)
    res[z, :, here] = (hp[...].reshape(64, 128).astype(F32) + attn).astype(BF16)
    mine = res.at[z, :, here]
    first = z // 2
    lean = 2 * (z % 2) - 1
    pairs = [lax.rem(first + lean * turn + 4, 4) for turn in PAIRS]
    for zt in [z - lean] + [2 * pair + k for pair in pairs[1:] for k in range(2)]:
        send(mine, mine, rz_s, rz_r.at[z], {"z": zt})
    for device in ys:
        send(mine, mine, ry_s, ry_r.at[kv], device)

    rows = pl.ds(pl.multiple_of(y * 16, 16), 16)

    def two(pair):
        return pl.ds(pl.multiple_of(2 * pair, 2), 2)

    def relay(pair):
        for k in range(2):
            zt = 2 * pair + k
            piece = res.at[zt, :, here]

            @pl.when(zt != z)
            def _():
                wait(piece, rz_r.at[zt])
                for device in ys:
                    send(piece, piece, ry_s, ry_r.at[NY * zt + y], device)

    def raise_up(pair):
        for k in range(2):
            zt = 2 * pair + k
            for dy in (1, 3, 2):
                yt = around(y, dy, NY)
                wait(res.at[zt, :, lanes(yt, 128)], ry_r.at[NY * zt + yt])
        both = res[two(pair)].reshape(128, 512).astype(F32)
        fed = (both * mlp_gain[...].astype(F32).reshape(1, 512)).astype(BF16)
        part = jnp.dot(fed, wu[...], preferred_element_type=F32).astype(BF16)
        upb[two(pair)] = part.reshape(2, 64, 512)
        send(upb.at[2 * pair + 1 - c], dd.at[pair], dd_s, dd_r.at[pair], {"c": 1 - c})

    def squares():
        own = res[z, rows, :].astype(F32)
        sq2[tp] = jnp.broadcast_to(jnp.sum(own * own, axis=-1, keepdims=True), (16, 128))
        for device in tps:
            send(sq2.at[tp], sq2.at[tp], sq2_s, sq2_r, device)

    def across(pair):
        wait(dd.at[pair], dd_r.at[pair])
        total = upb[2 * pair + c].astype(F32) + dd[pair].astype(F32)
        us[pair] = total.astype(BF16).reshape(NX, 16, 512)
        for dx in (2, 1, 3):
            xs = around(x, dx, NX)
            send(us.at[pair, xs], ur.at[pair, x], us_s, us_r.at[pair], {"x": xs})

    def activate(pair):
        wait(ur.at[pair, pl.ds(0, 3)], us_r.at[pair])
        total = us[pair, x].astype(F32)
        for dx in (1, 3, 2):
            total = total + ur[pair, around(x, dx, NX)].astype(F32)
        act[2 * pair + c, x] = jnp.square(jnp.maximum(total, 0.0)).astype(BF16)
        piece = act.at[2 * pair + c, x]
        for dx in (2, 1, 3):
            send(piece, piece, ac_s, ac_r.at[pair], {"x": around(x, dx, NX)})

    def hand_over(pair):
        piece = act.at[2 * pair + c]
        wait(piece.at[pl.ds(0, 3)], ac_r.at[pair])
        send(piece, piece, ac_s, ad_r.at[pair], {"c": 1 - c})

    def bring_down(pair):
        wait(act.at[NC * pair + 1 - c], ad_r.at[pair])
        part = jnp.dot(act[two(pair)].reshape(128, 512), wdn[...], preferred_element_type=F32).astype(BF16)
        dp[two(pair)] = part.reshape(2, NY, 16, 512)
        for device in ys:
            send(dp.at[two(pair), device["y"]], dyb.at[y, two(pair)], dy_s, dy_r.at[pair], device)

    def settle(pair):
        wait(dyb.at[pl.ds(0, 3), two(pair)], dy_r.at[pair])
        total = dp[two(pair), y].astype(F32)
        for dy in (1, 2, 3):
            total = total + dyb[around(y, dy, NY), two(pair)].astype(F32)
        zs[two(pair)] = total.astype(BF16)
        for k in range(2):
            j = 2 * pair + k

            @pl.when(j != z)
            def _():
                send(zs.at[j], zr.at[z], zr_s, zr_r, {"z": j})

    stages = (
        (0.0, relay), (2.0, raise_up), (3.1, across), (5.2, activate), (7.3, hand_over), (8.4, bring_down), (10.5, settle),
    )
    gaps = [(5, 1), (5, 2), (6, 2), (6, 3)]
    order = sorted((offset + turn, stage, turn) for stage, (offset, _) in enumerate(stages) for turn in range(4))
    pltpu.make_async_copy(wu_hbm, wu, in_sem.at[1]).wait()
    pltpu.make_async_copy(wdn_hbm, wdn, in_sem.at[2]).wait()
    for _, stage, turn in order:
        if (stage, turn) in gaps:
            renew(gaps.index((stage, turn)), 1)
        stages[stage][1](pairs[turn])
        if stage == 1 and turn == 0:
            squares()

    zr[z] = zs[z]
    renew(4, 4)
    wait(sq2.at[pl.ds(0, 7)], sq2_r)
    wait(zr.at[pl.ds(0, 7)], zr_r)
    mean = jnp.sum(sq2[...], axis=0)[:, 0:1] / D
    squared = 1.0 / (mean + EPS)
    mlp = (jnp.sum(zr[...].astype(F32), axis=0) * squared).astype(BF16).astype(F32)
    out[...] = (res[z, rows, :].astype(F32) + mlp).astype(BF16)

    wait(hx.at[pl.ds(0, 3)], hx_s)
    wait(sq.at[pl.ds(0, 7)], sq_s)
    for number in range(14):
        wait(slot(0, 0), wo_s.at[number])
    for number, (home, array, columns) in enumerate(pieces):

        @pl.when(y != home)
        def _():
            wait(wb.at[0, :, columns], wb_s.at[number])

    for dx in range(NX):
        wait(half(hx, 0, 0), zb_s.at[2 * dx + 1])

        @pl.when(NC * around(x, dx, NX) + c != z)
        def _():
            wait(half(hx, 0, 0), zb_s.at[2 * dx])

    wait(xb.at[pl.ds(0, 28)], yb_s)

    by_width(lambda width: wait(pb.at[pl.ds(0, 19), :, slice(0, width)], rb_s))
    by_width(lambda width: wait(pb.at[pl.ds(0, 12), :, slice(0, width)], rl_s))

    wait(mb.at[pl.ds(0, 3)], mb_s)
    wait(hp.at[pl.ds(0, 3)], hp_s)
    wait(r2.at[pl.ds(0, 7)], op_s)
    wait(op.at[pl.ds(0, 7)], rz_s)
    wait(res.at[:, :, slice(0, 384)], ry_s)
    wait(sq2.at[pl.ds(0, 7)], sq2_s)
    wait(dd, dd_s)
    wait(us.at[pl.ds(0, 3)], us_s)
    wait(act.at[pl.ds(0, 7)], ac_s)
    wait(dyb.at[pl.ds(0, 3)], dy_s)
    wait(zr.at[pl.ds(0, 7)], zr_s)


def body(
    hidden_rows, carried_state, norm_gain, w_query, w_key, w_decay, w_value, w_gate,
    decay_bias, head_gain, w_out, mlp_gain, w_up, w_down,
):
    dma = pltpu.SemaphoreType.DMA
    vmem = pl.BlockSpec(memory_space=pltpu.VMEM)
    return pl.pallas_call(
        layer_kernel,
        out_shape=(pltpu.VMEM((16, 512), BF16), pltpu.VMEM((16, 65536), F32)),
        in_specs=[pl.BlockSpec(memory_space=pltpu.HBM)] * 14,
        out_specs=(vmem, vmem),
        scratch_shapes=[
            pltpu.VMEM((16, 512), BF16),
            pltpu.VMEM((4096,), BF16),
            pltpu.VMEM((256,), F32),
            pltpu.VMEM((256,), BF16),
            pltpu.VMEM((512,), BF16),
            pltpu.VMEM((NX, 16, 512), BF16),
            pltpu.VMEM((8, 16, 128), F32),
            pltpu.VMEM((32, 16, 512), BF16),
            pltpu.VMEM((NY, 128, 512), BF16),
            pltpu.VMEM((32, 16, 512), BF16),
            pltpu.VMEM((NY, 5, 16, 512), BF16),
            pltpu.VMEM((3, NY, 16, 512), BF16),
            pltpu.VMEM((16, 1792), F32),
            pltpu.VMEM((512, 1024), BF16),
            pltpu.VMEM((16, 65536), F32),
            pltpu.VMEM((16, 512), F32),
            pltpu.VMEM((16, 256), F32),
            pltpu.VMEM((16, 256), F32),
            pltpu.VMEM((512, 512), BF16),
            pltpu.VMEM((512, 512), BF16),
            pltpu.VMEM((NY, 16, 512), BF16),
            pltpu.VMEM((NY, 16, 128), BF16),
            pltpu.VMEM((8, 64, 128), BF16),
            pltpu.VMEM((8, 64, 128), BF16),
            pltpu.VMEM((NZ, 64, 512), BF16),
            pltpu.VMEM((8, 16, 128), F32),
            pltpu.VMEM((8, 64, 512), BF16),
            pltpu.VMEM((4, 64, 512), BF16),
            pltpu.VMEM((4, NX, 16, 512), BF16),
            pltpu.VMEM((4, NX, 16, 512), BF16),
            pltpu.VMEM((8, NX, 16, 512), BF16),
            pltpu.VMEM((8, NY, 16, 512), BF16),
            pltpu.VMEM((NY, 8, 16, 512), BF16),
            pltpu.VMEM((8, 16, 512), BF16),
            pltpu.VMEM((NZ, 16, 512), BF16),
            dma((9,)), dma, dma((NX,)), dma, dma, dma((8,)), dma((NZ,)), dma, dma((32,)), dma((NZ,)),
            dma((5,)), dma, dma((14,)), dma((2, NZ)), dma, dma((NY,)), dma, dma((3,)),
            dma, dma, dma, dma, dma, dma, dma, dma((NZ,)), dma, dma((32,)), dma, dma,
            dma, dma((4,)), dma, dma((4,)), dma, dma((4,)), dma((4,)), dma, dma((4,)), dma, dma,
        ],
        compiler_params=pltpu.CompilerParams(collective_id=0, has_side_effects=True, vmem_limit_bytes=(59 << 20) + (800 << 10)),
        name="layer",
    )(
        hidden_rows, norm_gain, decay_bias, head_gain, mlp_gain, w_query, w_key, w_decay, w_value, w_gate,
        w_out, w_up, w_down, carried_state,
    )


def solution(mesh):
    finer = Mesh(mesh.devices.reshape(NZ, NY, NX, NC), ("z", "y", "x", "c"))
    placed = (
        P(KV, TP), P(KV, TP), P(), P(KV, TP), P(KV, TP), P(KV, TP), P(KV, TP), P(KV, TP),
        P(TP), P(), P(TP, KV), P(TP), P(TP, KV), P(KV, TP),
    )
    return jax.shard_map(
        body, mesh=finer, in_specs=placed, out_specs=(P(KV, TP), P(KV, TP)), check_vma=False
    )
```

```python
import jax
import jax.numpy as jnp
from jax import lax
from jax.experimental import pallas as pl
from jax.experimental.pallas import tpu as pltpu
from jax.sharding import Mesh
from jax.sharding import PartitionSpec as P

D = 4096
DK = 128
DV = 256
EPS = 1e-06
MESH = pl.DeviceIdType.MESH
F32 = jnp.float32
BF16 = jnp.bfloat16
KV = ("z", "y")
TP = ("x", "c")
NZ, NY, NX, NC = 8, 4, 4, 2
GROUPS = ((0, 1), (7, 2), (6, 3), (5, 4))
PAIRS = (0, 1, 2, 3)
KEYS = 32


def place():
    return tuple(lax.axis_index(name) for name in ("z", "y", "x", "c"))


def send(src, dst, sent, arrived, device):
    pltpu.make_async_remote_copy(
        src_ref=src, dst_ref=dst, send_sem=sent, recv_sem=arrived, device_id=device, device_id_type=MESH
    ).start()


def wait(ref, sem):
    pltpu.make_async_copy(ref, ref, sem).wait()


def greet(peers):
    for device in peers:
        pl.semaphore_signal(pltpu.get_barrier_semaphore(), inc=1, device_id=device, device_id_type=MESH)


def around(index, step, count):
    return lax.rem(index + step, count)


def layer_kernel(
    hid_hbm, norm_gain_hbm, bias_hbm, head_gain_hbm, mlp_gain_hbm,
    wq, wk, wd, wv, wg, wo, wu_hbm, wdn_hbm, state_hbm,
    out, new_state, hid, norm_gain, bias, head_gain, mlp_gain,
    hx, sq, xb, wb, pb, rb, rl, proj, wog, state, acc, decay, asked,
    wu, wdn, mb, hp, op, r2, res, sq2, upb, ur, act, dp, dyb, zs, zr,
    in_sem, hx_s, hx_r, sq_s, sq_r, zb_s, zb_r, yb_s, yb_r, db_r, wb_s, wb_r, wo_s, wo_r, rb_s, rb_r, rl_s, rl_r,
    mb_s, mb_r, hp_s, hp_r, op_s, op_r, rz_s, rz_r, ry_s, ry_r, sq2_s, sq2_r,
    us_s, us_r, ac_s, ac_r, ad_r, dy_s, dy_r, zr_s, zr_r,
):
    z, y, x, c = place()
    kv = NY * z + y
    tp = NC * x + c
    small = (
        (hid_hbm, hid), (norm_gain_hbm, norm_gain), (bias_hbm, bias), (head_gain_hbm, head_gain), (mlp_gain_hbm, mlp_gain),
    )
    for number, (src, dst) in enumerate(small):
        pltpu.make_async_copy(src, dst, in_sem.at[4 + number]).start()
    pltpu.make_async_copy(state_hbm, state, in_sem.at[0]).start()
    pltpu.make_async_copy(wu_hbm, wu, in_sem.at[1]).start()
    pltpu.make_async_copy(wdn_hbm, wdn, in_sem.at[2]).start()
    tps = [
        {"x": around(x, dx, NX), "c": around(c, dc, NC)} for dx in (2, 1, 3, 0) for dc in range(NC) if dx or dc
    ]
    ys = [{"y": around(y, dy, NY)} for dy in (2, 1, 3)]
    zfar = [{"z": around(z, dz, NZ)} for dz in (4, 3, 5, 2, 6, 1, 7)]
    peers = tps + zfar + [{"z": device["z"], "c": 1 - c} for device in zfar] + ys
    greet(peers)
    for number, (src, dst) in enumerate(small):
        pltpu.make_async_copy(src, dst, in_sem.at[4 + number]).wait()
    h = hid[...].astype(F32)
    gain = norm_gain[pl.ds(pl.multiple_of(tp * 512, 512), 512)].astype(F32).reshape(1, 512)
    hx[x] = (h * gain).astype(BF16)
    sq[tp] = jnp.broadcast_to(jnp.sum(h * h, axis=-1, keepdims=True), (16, 128))
    pl.semaphore_wait(pltpu.get_barrier_semaphore(), len(peers))

    def lanes(index, width):
        return pl.ds(pl.multiple_of(index * width, width), width)

    side = 1 - 2 * c

    def at(offset):
        return lax.rem(z + offset * side + NZ, NZ)

    def slot(origin, part):
        return wog.at[pl.ds(part * 256, 256), lanes(origin, 128)]

    for dx in (2, 1, 3):
        send(hx.at[x], hx.at[x], hx_s, hx_r.at[x], {"x": around(x, dx, NX)})
    for device in tps:
        send(sq.at[tp], sq.at[tp], sq_s, sq_r, device)
    up, down = around(z, 1, NZ), around(z, NZ - 1, NZ)
    for part in range(2):
        mine = wo.at[pl.ds(part * 256, 256)]
        send(mine, slot(z, part), wo_s.at[7 * part], wo_r.at[part, z], {"z": up})
        send(mine, slot(z, part), wo_s.at[7 * part + 1], wo_r.at[part, z], {"z": down})
    own_out = pltpu.make_async_copy(wo, wog.at[:, lanes(z, 128)], in_sem.at[3])
    own_out.start()
    pieces = (
        (0, wv, slice(0, 512)),
        (1, wg, slice(0, 512)),
        (2, wq, slice(0, 256)),
        (2, wk, slice(256, 512)),
        (3, wd, slice(0, 256)),
    )
    for number, (home, array, columns) in enumerate(pieces):
        target = wb.at[y, :, columns]

        @pl.when(y != home)
        def _():
            send(array, target, wb_s.at[number], wb_r, {"y": home})

        @pl.when(y == home)
        def _():
            pltpu.make_async_copy(array, target, wb_r).start()

    for dy in (2, 1, 3):
        yt = around(y, dy, NY)
        send(hid.at[:, lanes(yt, 128)], hp.at[y], hp_s, hp_r, {"y": yt})
    hp[y] = hid[:, lanes(y, 128)]

    def pass_on(step, part):
        low = around(z, NZ - step + 1, NZ)
        wait(slot(low, part), wo_r.at[part, low])
        send(slot(low, part), slot(low, part), wo_s.at[7 * part + 2 * step - 2], wo_r.at[part, low], {"z": up})
        high = around(z, step - 1, NZ)
        wait(slot(high, part), wo_r.at[part, high])
        if step < 4:
            send(slot(high, part), slot(high, part), wo_s.at[7 * part + 2 * step - 1], wo_r.at[part, high], {"z": down})

    def half(ref, number, which):
        return ref.at[number, :, lanes(which, 256)]

    for dx in (0, 1, 3, 2):
        xs = around(x, dx, NX)
        if dx:
            wait(hx.at[xs], hx_r.at[xs])
        zt = NC * xs + c
        for dc in range(NC):
            core = around(c, dc, NC)
            src, dst = half(hx, xs, core), half(xb, kv, core)
            if dc:
                send(src, dst, zb_s.at[2 * dx + dc], zb_r.at[z], {"z": zt, "c": core})
            else:

                @pl.when(zt != z)
                def _():
                    send(src, dst, zb_s.at[2 * dx], zb_r.at[z], {"z": zt, "c": core})

                @pl.when(zt == z)
                def _():
                    pltpu.make_async_copy(src, dst, zb_r.at[z]).start()

    def spread_y(group):
        for dz in group:
            zt = at(dz)
            number = NY * zt + y
            piece = half(xb, number, c)
            wait(piece, zb_r.at[zt])
            for device in ys:
                send(piece, piece, yb_s, yb_r.at[number], device)
            send(piece, piece, yb_s, db_r.at[zt], {"c": 1 - c})

    def spread_c(group):
        for dz in group:
            zt = at(dz)
            for dy in (1, 3, 2):
                number = NY * zt + around(y, dy, NY)
                piece = half(xb, number, c)
                wait(piece, yb_r.at[number])
                send(piece, piece, yb_s, db_r.at[zt], {"c": 1 - c})

    def plane(offset):
        return pl.ds(pl.multiple_of(NY * at(offset), NY), NY)

    def by_width(action):
        @pl.when(y < 3)
        def _():
            action(512)

        @pl.when(y == 3)
        def _():
            action(256)

    def scatter(offset, kind, width):
        for dy in (2, 1, 3, 0):
            yt = around(y, dy, NY)
            src = pb.at[NY * at(offset) + yt, :, slice(0, width)]
            dst = rb.at[y, kind, :, slice(0, width)]
            if offset or dy:
                send(src, dst, rb_s, rb_r.at[y], {"z": at(offset), "y": yt})
            else:
                pltpu.make_async_copy(src, dst, rb_r.at[y]).start()

    def lend(offset, number, via, width):
        src, dst = pb.at[plane(offset), :, slice(0, width)], rl.at[number, :, :, slice(0, width)]
        send(src, dst, rl_s, rl_r.at[number], {"z": at(via)})

    def combine(offset, number, kind, width):
        wait(rl.at[number, :, :, slice(0, width)], rl_r.at[number])
        total = pb[plane(offset), :, 0:width].astype(F32) + rl[number, :, :, 0:width].astype(F32)
        pb[plane(offset), :, 0:width] = total.astype(BF16)
        scatter(offset, kind, width)

    def multiply(group):
        for dz in group:
            wait(xb.at[plane(dz), :, slice(0, 256)], db_r.at[at(dz)])
        rows = [xb[plane(dz)].reshape(64, 512) for dz in group]
        weights = wb[...].reshape(512, 512)
        part = jnp.dot(jnp.concatenate(rows, axis=0), weights, preferred_element_type=F32).astype(BF16)
        for number, dz in enumerate(group):
            pb[plane(dz)] = part[64 * number : 64 * number + 64].reshape(NY, 16, 512)

    spread_y(GROUPS[0])
    pass_on(2, 0)
    spread_y(GROUPS[1])
    pass_on(2, 1)
    spread_y(GROUPS[2])
    spread_y(GROUPS[3])
    spread_c(GROUPS[0])
    pass_on(3, 0)
    spread_c(GROUPS[1])
    pass_on(3, 1)
    by_width(lambda width: wait(wb.at[:, :, slice(0, width)], wb_r))
    multiply(GROUPS[0])
    spread_c(GROUPS[2])
    by_width(lambda width: scatter(0, 0, width))
    multiply(GROUPS[1])
    spread_c(GROUPS[3])
    by_width(lambda width: lend(2, 0, 1, width))
    multiply(GROUPS[3])
    by_width(lambda width: (lend(4, 1, 1, width), lend(5, 2, 7, width), scatter(7, 4, width)))
    multiply(GROUPS[2])
    by_width(lambda width: combine(1, 0, 1, width))
    by_width(lambda width: combine(3, 1, 2, width))
    by_width(lambda width: combine(6, 2, 3, width))
    pass_on(4, 0)
    pass_on(4, 1)

    wait(sq.at[pl.ds(0, 7)], sq_r)
    scale = lax.rsqrt(jnp.sum(sq[...], axis=0) / D + EPS)[:, 0:1]

    def summed(block, width, offset):
        wait(rb.at[block, :, :, slice(0, width)], rb_r.at[block])
        total = jnp.sum(rb[block, :, :, 0:width].astype(F32), axis=0)
        proj[:, offset : offset + width] = (total * scale).astype(BF16).astype(F32)

    summed(3, 256, 0)
    summed(2, 512, 256)
    summed(0, 512, 768)
    summed(1, 512, 1280)
    pre = proj[:, 0:256] + bias[...].reshape(1, 256)
    soft = jnp.minimum(pre, 0.0) - jnp.log1p(jnp.exp(-jnp.abs(pre)))
    decay[...] = jnp.exp(soft / 16.0)
    acc[...] = jnp.zeros_like(acc)
    queries, keys_now = proj[:, 256:512] * DK ** (-0.5), proj[:, 512:768]
    asked[...] = queries * decay[...]
    for head in range(2):
        columns = slice(head * DK, head * DK + DK)
        meet = jnp.sum(queries[:, columns] * keys_now[:, columns], axis=-1, keepdims=True)
        acc[:, head * DV : head * DV + DV] = meet * proj[:, 768 + head * DV : 768 + head * DV + DV]
    pltpu.make_async_copy(state_hbm, state, in_sem.at[0]).wait()

    def turned(ref, step):
        return pltpu.roll(ref, lax.rem(256 - step * KEYS, 256), axis=1)

    for head in range(2):
        columns = slice(head * DV, head * DV + DV)
        totals = [acc[:, columns]] + [jnp.zeros((16, DV), F32)] * 3
        for key in range(head * DK, head * DK + DK):
            weight = asked[:, key : key + 1]
            totals[key % 4] = totals[key % 4] + weight * state[:, key * DV : key * DV + DV]
        acc[:, columns] = (totals[0] + totals[1]) + (totals[2] + totals[3])

    def renew(first_step, steps):
        @pl.loop(first_step, first_step + steps)
        def _(step):
            rates = turned(decay[...], step)
            keys = turned(proj[:, 512:768], step)
            values = proj[:, pl.ds(pl.multiple_of(768 + step // (DK // KEYS) * DV, DV), DV)]
            for key in range(KEYS):
                where = pl.ds(pl.multiple_of((step * KEYS + key) * DV, DV), DV)
                new_state[:, where] = rates[:, key : key + 1] * state[:, where] + keys[:, key : key + 1] * values

    for number in range(2):
        part = slice(number * DV, number * DV + DV)
        value = acc[:, part]
        gate = proj[:, 1280 + number * DV : 1280 + number * DV + DV]
        normal = value * lax.rsqrt(jnp.mean(value * value, axis=-1, keepdims=True) + EPS)
        silu = gate / (1.0 + jnp.exp(-gate))
        mb[y, :, part] = (normal * head_gain[...].astype(F32).reshape(1, DV) * silu).astype(BF16)
    for device in ys:
        send(mb.at[y], mb.at[y], mb_s, mb_r, device)
    here = lanes(y, 128)
    last = around(z, 4, NZ)
    for part in range(2):
        wait(slot(last, part), wo_r.at[part, last])
    own_out.wait()
    wait(mb.at[pl.ds(0, 3)], mb_r)
    part = jnp.dot(mb[...].reshape(64, 512), wog[...], preferred_element_type=F32).astype(BF16)
    for t in range(8):
        op[t] = part[:, t * 128 : t * 128 + 128]
    r2[tp] = op[tp]
    for device in tps:
        t = NC * device["x"] + device["c"]
        send(op.at[t], r2.at[tp], op_s, op_r, device)
    wait(hp.at[pl.ds(0, 3)], hp_r)
    wait(r2.at[pl.ds(0, 7)], op_r)
    attn = jnp.sum(r2[...].astype(F32), axis=0).astype(BF16).astype(F32)
    res[z, :, here] = (hp[...].reshape(64, 128).astype(F32) + attn).astype(BF16)
    mine = res.at[z, :, here]
    first = z // 2
    lean = 2 * (z % 2) - 1
    pairs = [lax.rem(first + lean * turn + 4, 4) for turn in PAIRS]
    for zt in [z - lean] + [2 * pair + k for pair in pairs[1:] for k in range(2)]:
        send(mine, mine, rz_s, rz_r.at[z], {"z": zt})
    for device in ys:
        send(mine, mine, ry_s, ry_r.at[kv], device)

    rows = pl.ds(pl.multiple_of(y * 16, 16), 16)

    def two(pair):
        return pl.ds(pl.multiple_of(2 * pair, 2), 2)

    def relay(pair):
        for k in range(2):
            zt = 2 * pair + k
            piece = res.at[zt, :, here]

            @pl.when(zt != z)
            def _():
                wait(piece, rz_r.at[zt])
                for device in ys:
                    send(piece, piece, ry_s, ry_r.at[NY * zt + y], device)

    def raise_up(pair):
        for k in range(2):
            zt = 2 * pair + k
            for dy in (1, 3, 2):
                yt = around(y, dy, NY)
                wait(res.at[zt, :, lanes(yt, 128)], ry_r.at[NY * zt + yt])
        both = res[two(pair)].reshape(128, 512).astype(F32)
        fed = (both * mlp_gain[...].astype(F32).reshape(1, 512)).astype(BF16)
        part = jnp.dot(fed, wu[...], preferred_element_type=F32).astype(BF16)
        upb[two(pair)] = part.reshape(2, NX, 16, 512)
        for device in tps:
            src = upb.at[2 * pair + device["c"], device["x"]]
            send(src, ur.at[pair, tp], us_s, us_r.at[pair], device)

    def squares():
        own = res[z, rows, :].astype(F32)
        sq2[tp] = jnp.broadcast_to(jnp.sum(own * own, axis=-1, keepdims=True), (16, 128))
        for device in tps:
            send(sq2.at[tp], sq2.at[tp], sq2_s, sq2_r, device)

    def activate(pair):
        ur[pair, tp] = upb[2 * pair + c, x]
        wait(ur.at[pair, pl.ds(0, 7)], us_r.at[pair])
        total = jnp.sum(ur[pair].astype(F32), axis=0)
        act[2 * pair + c, x] = jnp.square(jnp.maximum(total, 0.0)).astype(BF16)
        piece = act.at[2 * pair + c, x]
        for dx in (2, 1, 3):
            send(piece, piece, ac_s, ac_r.at[pair], {"x": around(x, dx, NX)})

    def hand_over(pair):
        piece = act.at[2 * pair + c]
        wait(piece.at[pl.ds(0, 3)], ac_r.at[pair])
        send(piece, piece, ac_s, ad_r.at[pair], {"c": 1 - c})

    def bring_down(pair):
        wait(act.at[NC * pair + 1 - c], ad_r.at[pair])
        part = jnp.dot(act[two(pair)].reshape(128, 512), wdn[...], preferred_element_type=F32).astype(BF16)
        dp[two(pair)] = part.reshape(2, NY, 16, 512)
        for device in ys:
            send(dp.at[two(pair), device["y"]], dyb.at[y, two(pair)], dy_s, dy_r.at[pair], device)

    def settle(pair):
        wait(dyb.at[pl.ds(0, 3), two(pair)], dy_r.at[pair])
        total = dp[two(pair), y].astype(F32)
        for dy in (1, 2, 3):
            total = total + dyb[around(y, dy, NY), two(pair)].astype(F32)
        zs[two(pair)] = total.astype(BF16)
        for k in range(2):
            j = 2 * pair + k

            @pl.when(j != z)
            def _():
                send(zs.at[j], zr.at[z], zr_s, zr_r, {"z": j})

    stages = (
        (0.0, relay), (2.0, raise_up), (5.2, activate), (7.3, hand_over), (8.4, bring_down), (10.5, settle),
    )
    gaps = [(4, 1), (4, 2), (5, 2), (5, 3)]
    order = sorted((offset + turn, stage, turn) for stage, (offset, _) in enumerate(stages) for turn in range(4))
    pltpu.make_async_copy(wu_hbm, wu, in_sem.at[1]).wait()
    pltpu.make_async_copy(wdn_hbm, wdn, in_sem.at[2]).wait()
    for _, stage, turn in order:
        if (stage, turn) in gaps:
            renew(gaps.index((stage, turn)), 1)
        stages[stage][1](pairs[turn])
        if stage == 1 and turn == 0:
            squares()

    zr[z] = zs[z]
    renew(4, 4)
    wait(sq2.at[pl.ds(0, 7)], sq2_r)
    wait(zr.at[pl.ds(0, 7)], zr_r)
    mean = jnp.sum(sq2[...], axis=0)[:, 0:1] / D
    squared = 1.0 / (mean + EPS)
    mlp = (jnp.sum(zr[...].astype(F32), axis=0) * squared).astype(BF16).astype(F32)
    out[...] = (res[z, rows, :].astype(F32) + mlp).astype(BF16)

    wait(hx.at[pl.ds(0, 3)], hx_s)
    wait(sq.at[pl.ds(0, 7)], sq_s)
    for number in range(14):
        wait(slot(0, 0), wo_s.at[number])
    for number, (home, array, columns) in enumerate(pieces):

        @pl.when(y != home)
        def _():
            wait(wb.at[0, :, columns], wb_s.at[number])

    for dx in range(NX):
        wait(half(hx, 0, 0), zb_s.at[2 * dx + 1])

        @pl.when(NC * around(x, dx, NX) + c != z)
        def _():
            wait(half(hx, 0, 0), zb_s.at[2 * dx])

    wait(xb.at[pl.ds(0, 28)], yb_s)

    by_width(lambda width: wait(pb.at[pl.ds(0, 19), :, slice(0, width)], rb_s))
    by_width(lambda width: wait(pb.at[pl.ds(0, 12), :, slice(0, width)], rl_s))

    wait(mb.at[pl.ds(0, 3)], mb_s)
    wait(hp.at[pl.ds(0, 3)], hp_s)
    wait(r2.at[pl.ds(0, 7)], op_s)
    wait(op.at[pl.ds(0, 7)], rz_s)
    wait(res.at[:, :, slice(0, 384)], ry_s)
    wait(sq2.at[pl.ds(0, 7)], sq2_s)
    wait(ur.at[:, pl.ds(0, 7)], us_s)
    wait(act.at[pl.ds(0, 7)], ac_s)
    wait(dyb.at[pl.ds(0, 3)], dy_s)
    wait(zr.at[pl.ds(0, 7)], zr_s)


PARTS = 8


def flush_kernel(out, state, out_hbm, state_hbm, sem):
    wide = state.shape[1] // PARTS
    copies = [pltpu.make_async_copy(out, out_hbm, sem.at[PARTS])]
    for number in range(PARTS):
        part = pl.ds(number * wide, wide)
        copies.append(pltpu.make_async_copy(state.at[:, part], state_hbm.at[:, part], sem.at[number]))
    for copy in copies:
        copy.start()
    for copy in copies:
        copy.wait()


def flush(out, state):
    vmem = pl.BlockSpec(memory_space=pltpu.VMEM)
    hbm = pl.BlockSpec(memory_space=pltpu.HBM)
    return pl.pallas_call(
        flush_kernel,
        out_shape=(jax.ShapeDtypeStruct(out.shape, out.dtype), jax.ShapeDtypeStruct(state.shape, state.dtype)),
        in_specs=[vmem, vmem],
        out_specs=(hbm, hbm),
        scratch_shapes=[pltpu.SemaphoreType.DMA((PARTS + 1,))],
        compiler_params=pltpu.CompilerParams(vmem_limit_bytes=1 << 20),
        name="flush",
    )(out, state)


def body(
    hidden_rows, carried_state, norm_gain, w_query, w_key, w_decay, w_value, w_gate,
    decay_bias, head_gain, w_out, mlp_gain, w_up, w_down,
):
    dma = pltpu.SemaphoreType.DMA
    vmem = pl.BlockSpec(memory_space=pltpu.VMEM)
    out, state = pl.pallas_call(
        layer_kernel,
        out_shape=(pltpu.VMEM((16, 512), BF16), pltpu.VMEM((16, 65536), F32)),
        in_specs=[pl.BlockSpec(memory_space=pltpu.HBM)] * 14,
        out_specs=(vmem, vmem),
        scratch_shapes=[
            pltpu.VMEM((16, 512), BF16),
            pltpu.VMEM((4096,), BF16),
            pltpu.VMEM((256,), F32),
            pltpu.VMEM((256,), BF16),
            pltpu.VMEM((512,), BF16),
            pltpu.VMEM((NX, 16, 512), BF16),
            pltpu.VMEM((8, 16, 128), F32),
            pltpu.VMEM((32, 16, 512), BF16),
            pltpu.VMEM((NY, 128, 512), BF16),
            pltpu.VMEM((32, 16, 512), BF16),
            pltpu.VMEM((NY, 5, 16, 512), BF16),
            pltpu.VMEM((3, NY, 16, 512), BF16),
            pltpu.VMEM((16, 1792), F32),
            pltpu.VMEM((512, 1024), BF16),
            pltpu.VMEM((16, 65536), F32),
            pltpu.VMEM((16, 512), F32),
            pltpu.VMEM((16, 256), F32),
            pltpu.VMEM((16, 256), F32),
            pltpu.VMEM((512, 512), BF16),
            pltpu.VMEM((512, 512), BF16),
            pltpu.VMEM((NY, 16, 512), BF16),
            pltpu.VMEM((NY, 16, 128), BF16),
            pltpu.VMEM((8, 64, 128), BF16),
            pltpu.VMEM((8, 64, 128), BF16),
            pltpu.VMEM((NZ, 64, 512), BF16),
            pltpu.VMEM((8, 16, 128), F32),
            pltpu.VMEM((8, NX, 16, 512), BF16),
            pltpu.VMEM((4, 8, 16, 512), BF16),
            pltpu.VMEM((8, NX, 16, 512), BF16),
            pltpu.VMEM((8, NY, 16, 512), BF16),
            pltpu.VMEM((NY, 8, 16, 512), BF16),
            pltpu.VMEM((8, 16, 512), BF16),
            pltpu.VMEM((NZ, 16, 512), BF16),
            dma((9,)), dma, dma((NX,)), dma, dma, dma((8,)), dma((NZ,)), dma, dma((32,)), dma((NZ,)),
            dma((5,)), dma, dma((14,)), dma((2, NZ)), dma, dma((NY,)), dma, dma((3,)),
            dma, dma, dma, dma, dma, dma, dma, dma((NZ,)), dma, dma((32,)), dma, dma,
            dma, dma((4,)), dma, dma((4,)), dma((4,)), dma, dma((4,)), dma, dma,
        ],
        compiler_params=pltpu.CompilerParams(collective_id=0, has_side_effects=True, vmem_limit_bytes=(59 << 20) + (800 << 10)),
        name="layer",
    )(
        hidden_rows, norm_gain, decay_bias, head_gain, mlp_gain, w_query, w_key, w_decay, w_value, w_gate,
        w_out, w_up, w_down, carried_state,
    )
    return flush(out, state)


def solution(mesh):
    finer = Mesh(mesh.devices.reshape(NZ, NY, NX, NC), ("z", "y", "x", "c"))
    placed = (
        P(KV, TP), P(KV, TP), P(), P(KV, TP), P(KV, TP), P(KV, TP), P(KV, TP), P(KV, TP),
        P(TP), P(), P(TP, KV), P(TP), P(TP, KV), P(KV, TP),
    )
    return jax.shard_map(
        body, mesh=finer, in_specs=placed, out_specs=(P(KV, TP), P(KV, TP)), check_vma=False
    )
```

```python
import jax
import jax.numpy as jnp
from jax import lax
from jax.experimental import pallas as pl
from jax.experimental.pallas import tpu as pltpu
from jax.sharding import Mesh
from jax.sharding import PartitionSpec as P

D = 4096
DK = 128
DV = 256
EPS = 1e-06
MESH = pl.DeviceIdType.MESH
F32 = jnp.float32
BF16 = jnp.bfloat16
KV = ("z", "y")
TP = ("x", "c")
NZ, NY, NX, NC = 8, 4, 4, 2
GROUPS = ((0, 1), (7, 2), (6, 3), (5, 4))
PAIRS = (0, 1, 2, 3)
KEYS = 32


def place():
    return tuple(lax.axis_index(name) for name in ("z", "y", "x", "c"))


def send(src, dst, sent, arrived, device):
    pltpu.make_async_remote_copy(
        src_ref=src, dst_ref=dst, send_sem=sent, recv_sem=arrived, device_id=device, device_id_type=MESH
    ).start()


def wait(ref, sem):
    pltpu.make_async_copy(ref, ref, sem).wait()


def greet(peers):
    for device in peers:
        pl.semaphore_signal(pltpu.get_barrier_semaphore(), inc=1, device_id=device, device_id_type=MESH)


def around(index, step, count):
    return lax.rem(index + step, count)


def layer_kernel(
    hid_hbm, norm_gain_hbm, bias_hbm, head_gain_hbm, mlp_gain_hbm,
    wq, wk, wd, wv, wg, wo, wu_hbm, wdn_hbm, state_hbm,
    out, new_state, hid, norm_gain, bias, head_gain, mlp_gain,
    hx, sq, xb, wb, pb, rb, rl, proj, wog, state, acc, decay, asked,
    wu, wdn, mb, hp, op, r2, res, sq2, upb, ur, act, dp, dyb, zs, zr,
    in_sem, hx_s, hx_r, sq_s, sq_r, zb_s, zb_r, yb_s, yb_r, db_r, wb_s, wb_r, wo_s, wo_r, rb_s, rb_r, rl_s, rl_r,
    mb_s, mb_r, hp_s, hp_r, op_s, op_r, rz_s, rz_r, ry_s, ry_r, sq2_s, sq2_r,
    us_s, us_r, ac_s, ac_r, ad_r, dy_s, dy_r, zr_s, zr_r,
):
    z, y, x, c = place()
    kv = NY * z + y
    tp = NC * x + c
    small = (
        (hid_hbm, hid), (norm_gain_hbm, norm_gain), (bias_hbm, bias), (head_gain_hbm, head_gain), (mlp_gain_hbm, mlp_gain),
    )
    for number, (src, dst) in enumerate(small):
        pltpu.make_async_copy(src, dst, in_sem.at[4 + number]).start()
    pltpu.make_async_copy(state_hbm, state, in_sem.at[0]).start()
    pltpu.make_async_copy(wu_hbm, wu, in_sem.at[1]).start()
    pltpu.make_async_copy(wdn_hbm, wdn, in_sem.at[2]).start()
    tps = [
        {"x": around(x, dx, NX), "c": around(c, dc, NC)} for dx in (2, 1, 3, 0) for dc in range(NC) if dx or dc
    ]
    ys = [{"y": around(y, dy, NY)} for dy in (2, 1, 3)]
    zfar = [{"z": around(z, dz, NZ)} for dz in (4, 3, 5, 2, 6, 1, 7)]
    peers = tps + zfar + [{"z": device["z"], "c": 1 - c} for device in zfar] + ys
    greet(peers)
    for number, (src, dst) in enumerate(small):
        pltpu.make_async_copy(src, dst, in_sem.at[4 + number]).wait()
    h = hid[...].astype(F32)
    gain = norm_gain[pl.ds(pl.multiple_of(tp * 512, 512), 512)].astype(F32).reshape(1, 512)
    hx[x] = (h * gain).astype(BF16)
    sq[tp] = jnp.broadcast_to(jnp.sum(h * h, axis=-1, keepdims=True), (16, 128))
    pl.semaphore_wait(pltpu.get_barrier_semaphore(), len(peers))

    def lanes(index, width):
        return pl.ds(pl.multiple_of(index * width, width), width)

    side = 1 - 2 * c

    def at(offset):
        return lax.rem(z + offset * side + NZ, NZ)

    def slot(origin, part):
        return wog.at[pl.ds(part * 256, 256), lanes(origin, 128)]

    for dx in (2, 1, 3):
        send(hx.at[x], hx.at[x], hx_s, hx_r.at[x], {"x": around(x, dx, NX)})
    for device in tps:
        send(sq.at[tp], sq.at[tp], sq_s, sq_r, device)
    up, down = around(z, 1, NZ), around(z, NZ - 1, NZ)
    for part in range(2):
        mine = wo.at[pl.ds(part * 256, 256)]
        send(mine, slot(z, part), wo_s.at[7 * part], wo_r.at[part, z], {"z": up})
        send(mine, slot(z, part), wo_s.at[7 * part + 1], wo_r.at[part, z], {"z": down})
    own_out = pltpu.make_async_copy(wo, wog.at[:, lanes(z, 128)], in_sem.at[3])
    own_out.start()
    pieces = (
        (0, wv, slice(0, 512)),
        (1, wg, slice(0, 512)),
        (2, wq, slice(0, 256)),
        (2, wk, slice(256, 512)),
        (3, wd, slice(0, 256)),
    )
    for number, (home, array, columns) in enumerate(pieces):
        target = wb.at[y, :, columns]

        @pl.when(y != home)
        def _():
            send(array, target, wb_s.at[number], wb_r, {"y": home})

        @pl.when(y == home)
        def _():
            pltpu.make_async_copy(array, target, wb_r).start()

    for dy in (2, 1, 3):
        yt = around(y, dy, NY)
        send(hid.at[:, lanes(yt, 128)], hp.at[y], hp_s, hp_r, {"y": yt})
    hp[y] = hid[:, lanes(y, 128)]

    def pass_on(step, part):
        low = around(z, NZ - step + 1, NZ)
        wait(slot(low, part), wo_r.at[part, low])
        send(slot(low, part), slot(low, part), wo_s.at[7 * part + 2 * step - 2], wo_r.at[part, low], {"z": up})
        high = around(z, step - 1, NZ)
        wait(slot(high, part), wo_r.at[part, high])
        if step < 4:
            send(slot(high, part), slot(high, part), wo_s.at[7 * part + 2 * step - 1], wo_r.at[part, high], {"z": down})

    def half(ref, number, which):
        return ref.at[number, :, lanes(which, 256)]

    for dx in (0, 1, 3, 2):
        xs = around(x, dx, NX)
        if dx:
            wait(hx.at[xs], hx_r.at[xs])
        zt = NC * xs + c
        for dc in range(NC):
            core = around(c, dc, NC)
            src, dst = half(hx, xs, core), half(xb, kv, core)
            if dc:
                send(src, dst, zb_s.at[2 * dx + dc], zb_r.at[z], {"z": zt, "c": core})
            else:

                @pl.when(zt != z)
                def _():
                    send(src, dst, zb_s.at[2 * dx], zb_r.at[z], {"z": zt, "c": core})

                @pl.when(zt == z)
                def _():
                    pltpu.make_async_copy(src, dst, zb_r.at[z]).start()

    def spread_y(group):
        for dz in group:
            zt = at(dz)
            number = NY * zt + y
            piece = half(xb, number, c)
            wait(piece, zb_r.at[zt])
            for device in ys:
                send(piece, piece, yb_s, yb_r.at[number], device)
            send(piece, piece, yb_s, db_r.at[zt], {"c": 1 - c})

    def spread_c(group):
        for dz in group:
            zt = at(dz)
            for dy in (1, 3, 2):
                number = NY * zt + around(y, dy, NY)
                piece = half(xb, number, c)
                wait(piece, yb_r.at[number])
                send(piece, piece, yb_s, db_r.at[zt], {"c": 1 - c})

    def plane(offset):
        return pl.ds(pl.multiple_of(NY * at(offset), NY), NY)

    def by_width(action):
        @pl.when(y < 3)
        def _():
            action(512)

        @pl.when(y == 3)
        def _():
            action(256)

    def scatter(offset, kind, width):
        for dy in (2, 1, 3, 0):
            yt = around(y, dy, NY)
            src = pb.at[NY * at(offset) + yt, :, slice(0, width)]
            dst = rb.at[y, kind, :, slice(0, width)]
            if offset or dy:
                send(src, dst, rb_s, rb_r.at[y], {"z": at(offset), "y": yt})
            else:
                pltpu.make_async_copy(src, dst, rb_r.at[y]).start()

    def lend(offset, number, via, width):
        src, dst = pb.at[plane(offset), :, slice(0, width)], rl.at[number, :, :, slice(0, width)]
        send(src, dst, rl_s, rl_r.at[number], {"z": at(via)})

    def combine(offset, number, kind, width):
        wait(rl.at[number, :, :, slice(0, width)], rl_r.at[number])
        total = pb[plane(offset), :, 0:width].astype(F32) + rl[number, :, :, 0:width].astype(F32)
        pb[plane(offset), :, 0:width] = total.astype(BF16)
        scatter(offset, kind, width)

    def multiply(group):
        for dz in group:
            wait(xb.at[plane(dz), :, slice(0, 256)], db_r.at[at(dz)])
        rows = [xb[plane(dz)].reshape(64, 512) for dz in group]
        weights = wb[...].reshape(512, 512)
        part = jnp.dot(jnp.concatenate(rows, axis=0), weights, preferred_element_type=F32).astype(BF16)
        for number, dz in enumerate(group):
            pb[plane(dz)] = part[64 * number : 64 * number + 64].reshape(NY, 16, 512)

    spread_y(GROUPS[0])
    pass_on(2, 0)
    spread_y(GROUPS[1])
    pass_on(2, 1)
    spread_y(GROUPS[2])
    spread_y(GROUPS[3])
    spread_c(GROUPS[0])
    pass_on(3, 0)
    spread_c(GROUPS[1])
    by_width(lambda width: wait(wb.at[:, :, slice(0, width)], wb_r))
    multiply(GROUPS[0])
    spread_c(GROUPS[2])
    pass_on(3, 1)
    by_width(lambda width: scatter(0, 0, width))
    multiply(GROUPS[1])
    spread_c(GROUPS[3])
    by_width(lambda width: lend(2, 0, 1, width))
    multiply(GROUPS[3])
    by_width(lambda width: (lend(4, 1, 1, width), lend(5, 2, 7, width), scatter(7, 4, width)))
    multiply(GROUPS[2])
    by_width(lambda width: combine(1, 0, 1, width))
    by_width(lambda width: combine(3, 1, 2, width))
    by_width(lambda width: combine(6, 2, 3, width))
    pass_on(4, 0)
    pass_on(4, 1)

    wait(sq.at[pl.ds(0, 7)], sq_r)
    scale = lax.rsqrt(jnp.sum(sq[...], axis=0) / D + EPS)[:, 0:1]

    def summed(block, width, offset):
        wait(rb.at[block, :, :, slice(0, width)], rb_r.at[block])
        total = jnp.sum(rb[block, :, :, 0:width].astype(F32), axis=0)
        proj[:, offset : offset + width] = (total * scale).astype(BF16).astype(F32)

    summed(3, 256, 0)
    summed(2, 512, 256)
    summed(0, 512, 768)
    summed(1, 512, 1280)
    pre = proj[:, 0:256] + bias[...].reshape(1, 256)
    soft = jnp.minimum(pre, 0.0) - jnp.log1p(jnp.exp(-jnp.abs(pre)))
    decay[...] = jnp.exp(soft / 16.0)
    acc[...] = jnp.zeros_like(acc)
    queries, keys_now = proj[:, 256:512] * DK ** (-0.5), proj[:, 512:768]
    asked[...] = queries * decay[...]
    for head in range(2):
        columns = slice(head * DK, head * DK + DK)
        meet = jnp.sum(queries[:, columns] * keys_now[:, columns], axis=-1, keepdims=True)
        acc[:, head * DV : head * DV + DV] = meet * proj[:, 768 + head * DV : 768 + head * DV + DV]
    pltpu.make_async_copy(state_hbm, state, in_sem.at[0]).wait()

    def turned(ref, step):
        return pltpu.roll(ref, lax.rem(256 - step * KEYS, 256), axis=1)

    for head in range(2):
        columns = slice(head * DV, head * DV + DV)
        totals = [acc[:, columns]] + [jnp.zeros((16, DV), F32)] * 3
        for key in range(head * DK, head * DK + DK):
            weight = asked[:, key : key + 1]
            totals[key % 4] = totals[key % 4] + weight * state[:, key * DV : key * DV + DV]
        acc[:, columns] = (totals[0] + totals[1]) + (totals[2] + totals[3])

    def renew(first_step, steps):
        @pl.loop(first_step, first_step + steps)
        def _(step):
            rates = turned(decay[...], step)
            keys = turned(proj[:, 512:768], step)
            values = proj[:, pl.ds(pl.multiple_of(768 + step // (DK // KEYS) * DV, DV), DV)]
            for key in range(KEYS):
                where = pl.ds(pl.multiple_of((step * KEYS + key) * DV, DV), DV)
                new_state[:, where] = rates[:, key : key + 1] * state[:, where] + keys[:, key : key + 1] * values

    for number in range(2):
        part = slice(number * DV, number * DV + DV)
        value = acc[:, part]
        gate = proj[:, 1280 + number * DV : 1280 + number * DV + DV]
        normal = value * lax.rsqrt(jnp.mean(value * value, axis=-1, keepdims=True) + EPS)
        silu = gate / (1.0 + jnp.exp(-gate))
        mb[y, :, part] = (normal * head_gain[...].astype(F32).reshape(1, DV) * silu).astype(BF16)
    for device in ys:
        send(mb.at[y], mb.at[y], mb_s, mb_r, device)
    here = lanes(y, 128)
    last = around(z, 4, NZ)
    for part in range(2):
        wait(slot(last, part), wo_r.at[part, last])
    own_out.wait()
    wait(mb.at[pl.ds(0, 3)], mb_r)
    part = jnp.dot(mb[...].reshape(64, 512), wog[...], preferred_element_type=F32).astype(BF16)
    for t in range(8):
        op[t] = part[:, t * 128 : t * 128 + 128]
    r2[tp] = op[tp]
    for device in tps:
        t = NC * device["x"] + device["c"]
        send(op.at[t], r2.at[tp], op_s, op_r, device)
    wait(hp.at[pl.ds(0, 3)], hp_r)
    wait(r2.at[pl.ds(0, 7)], op_r)
    attn = jnp.sum(r2[...].astype(F32), axis=0).astype(BF16).astype(F32)
    res[z, :, here] = (hp[...].reshape(64, 128).astype(F32) + attn).astype(BF16)
    mine = res.at[z, :, here]
    first = z // 2
    lean = 2 * (z % 2) - 1
    pairs = [lax.rem(first + lean * turn + 4, 4) for turn in PAIRS]
    for zt in [z - lean] + [2 * pair + k for pair in pairs[1:] for k in range(2)]:
        send(mine, mine, rz_s, rz_r.at[z], {"z": zt})
    for device in ys:
        send(mine, mine, ry_s, ry_r.at[kv], device)

    rows = pl.ds(pl.multiple_of(y * 16, 16), 16)

    def two(pair):
        return pl.ds(pl.multiple_of(2 * pair, 2), 2)

    def relay(pair):
        for k in range(2):
            zt = 2 * pair + k
            piece = res.at[zt, :, here]

            @pl.when(zt != z)
            def _():
                wait(piece, rz_r.at[zt])
                for device in ys:
                    send(piece, piece, ry_s, ry_r.at[NY * zt + y], device)

    def raise_up(pair):
        for k in range(2):
            zt = 2 * pair + k
            for dy in (1, 3, 2):
                yt = around(y, dy, NY)
                wait(res.at[zt, :, lanes(yt, 128)], ry_r.at[NY * zt + yt])
        both = res[two(pair)].reshape(128, 512).astype(F32)
        fed = (both * mlp_gain[...].astype(F32).reshape(1, 512)).astype(BF16)
        part = jnp.dot(fed, wu[...], preferred_element_type=F32).astype(BF16)
        upb[two(pair)] = part.reshape(2, NX, 16, 512)
        for device in tps:
            src = upb.at[2 * pair + device["c"], device["x"]]
            send(src, ur.at[pair, tp], us_s, us_r.at[pair], device)

    def squares():
        own = res[z, rows, :].astype(F32)
        sq2[tp] = jnp.broadcast_to(jnp.sum(own * own, axis=-1, keepdims=True), (16, 128))
        for device in tps:
            send(sq2.at[tp], sq2.at[tp], sq2_s, sq2_r, device)

    def activate(pair):
        ur[pair, tp] = upb[2 * pair + c, x]
        wait(ur.at[pair, pl.ds(0, 7)], us_r.at[pair])
        total = jnp.sum(ur[pair].astype(F32), axis=0)
        act[2 * pair + c, x] = jnp.square(jnp.maximum(total, 0.0)).astype(BF16)
        piece = act.at[2 * pair + c, x]
        for dx in (2, 1, 3):
            send(piece, piece, ac_s, ac_r.at[pair], {"x": around(x, dx, NX)})

    def hand_over(pair):
        piece = act.at[2 * pair + c]
        wait(piece.at[pl.ds(0, 3)], ac_r.at[pair])
        send(piece, piece, ac_s, ad_r.at[pair], {"c": 1 - c})

    def bring_down(pair):
        wait(act.at[NC * pair + 1 - c], ad_r.at[pair])
        part = jnp.dot(act[two(pair)].reshape(128, 512), wdn[...], preferred_element_type=F32).astype(BF16)
        dp[two(pair)] = part.reshape(2, NY, 16, 512)
        for device in ys:
            send(dp.at[two(pair), device["y"]], dyb.at[y, two(pair)], dy_s, dy_r.at[pair], device)

    def settle(pair):
        wait(dyb.at[pl.ds(0, 3), two(pair)], dy_r.at[pair])
        total = dp[two(pair), y].astype(F32)
        for dy in (1, 2, 3):
            total = total + dyb[around(y, dy, NY), two(pair)].astype(F32)
        zs[two(pair)] = total.astype(BF16)
        for k in range(2):
            j = 2 * pair + k

            @pl.when(j != z)
            def _():
                send(zs.at[j], zr.at[z], zr_s, zr_r, {"z": j})

    stages = (
        (0.0, relay), (2.0, raise_up), (5.2, activate), (7.3, hand_over), (8.4, bring_down), (10.5, settle),
    )
    gaps = [(4, 1), (4, 2), (5, 2), (5, 3)]
    order = sorted((offset + turn, stage, turn) for stage, (offset, _) in enumerate(stages) for turn in range(4))
    pltpu.make_async_copy(wu_hbm, wu, in_sem.at[1]).wait()
    pltpu.make_async_copy(wdn_hbm, wdn, in_sem.at[2]).wait()
    for _, stage, turn in order:
        if (stage, turn) in gaps:
            renew(gaps.index((stage, turn)), 1)
        stages[stage][1](pairs[turn])
        if stage == 1 and turn == 0:
            squares()

    zr[z] = zs[z]
    renew(4, 4)
    wait(sq2.at[pl.ds(0, 7)], sq2_r)
    wait(zr.at[pl.ds(0, 7)], zr_r)
    mean = jnp.sum(sq2[...], axis=0)[:, 0:1] / D
    squared = 1.0 / (mean + EPS)
    mlp = (jnp.sum(zr[...].astype(F32), axis=0) * squared).astype(BF16).astype(F32)
    out[...] = (res[z, rows, :].astype(F32) + mlp).astype(BF16)

    wait(hx.at[pl.ds(0, 3)], hx_s)
    wait(sq.at[pl.ds(0, 7)], sq_s)
    for number in range(14):
        wait(slot(0, 0), wo_s.at[number])
    for number, (home, array, columns) in enumerate(pieces):

        @pl.when(y != home)
        def _():
            wait(wb.at[0, :, columns], wb_s.at[number])

    for dx in range(NX):
        wait(half(hx, 0, 0), zb_s.at[2 * dx + 1])

        @pl.when(NC * around(x, dx, NX) + c != z)
        def _():
            wait(half(hx, 0, 0), zb_s.at[2 * dx])

    wait(xb.at[pl.ds(0, 28)], yb_s)

    by_width(lambda width: wait(pb.at[pl.ds(0, 19), :, slice(0, width)], rb_s))
    by_width(lambda width: wait(pb.at[pl.ds(0, 12), :, slice(0, width)], rl_s))

    wait(mb.at[pl.ds(0, 3)], mb_s)
    wait(hp.at[pl.ds(0, 3)], hp_s)
    wait(r2.at[pl.ds(0, 7)], op_s)
    wait(op.at[pl.ds(0, 7)], rz_s)
    wait(res.at[:, :, slice(0, 384)], ry_s)
    wait(sq2.at[pl.ds(0, 7)], sq2_s)
    wait(ur.at[:, pl.ds(0, 7)], us_s)
    wait(act.at[pl.ds(0, 7)], ac_s)
    wait(dyb.at[pl.ds(0, 3)], dy_s)
    wait(zr.at[pl.ds(0, 7)], zr_s)


PARTS = 8


def flush_kernel(out, state, out_hbm, state_hbm, sem):
    wide = state.shape[1] // PARTS
    copies = [pltpu.make_async_copy(out, out_hbm, sem.at[PARTS])]
    for number in range(PARTS):
        part = pl.ds(number * wide, wide)
        copies.append(pltpu.make_async_copy(state.at[:, part], state_hbm.at[:, part], sem.at[number]))
    for copy in copies:
        copy.start()
    for copy in copies:
        copy.wait()


def flush(out, state):
    vmem = pl.BlockSpec(memory_space=pltpu.VMEM)
    hbm = pl.BlockSpec(memory_space=pltpu.HBM)
    return pl.pallas_call(
        flush_kernel,
        out_shape=(jax.ShapeDtypeStruct(out.shape, out.dtype), jax.ShapeDtypeStruct(state.shape, state.dtype)),
        in_specs=[vmem, vmem],
        out_specs=(hbm, hbm),
        scratch_shapes=[pltpu.SemaphoreType.DMA((PARTS + 1,))],
        compiler_params=pltpu.CompilerParams(vmem_limit_bytes=1 << 20),
        name="flush",
    )(out, state)


def body(
    hidden_rows, carried_state, norm_gain, w_query, w_key, w_decay, w_value, w_gate,
    decay_bias, head_gain, w_out, mlp_gain, w_up, w_down,
):
    dma = pltpu.SemaphoreType.DMA
    vmem = pl.BlockSpec(memory_space=pltpu.VMEM)
    out, state = pl.pallas_call(
        layer_kernel,
        out_shape=(pltpu.VMEM((16, 512), BF16), pltpu.VMEM((16, 65536), F32)),
        in_specs=[pl.BlockSpec(memory_space=pltpu.HBM)] * 14,
        out_specs=(vmem, vmem),
        scratch_shapes=[
            pltpu.VMEM((16, 512), BF16),
            pltpu.VMEM((4096,), BF16),
            pltpu.VMEM((256,), F32),
            pltpu.VMEM((256,), BF16),
            pltpu.VMEM((512,), BF16),
            pltpu.VMEM((NX, 16, 512), BF16),
            pltpu.VMEM((8, 16, 128), F32),
            pltpu.VMEM((32, 16, 512), BF16),
            pltpu.VMEM((NY, 128, 512), BF16),
            pltpu.VMEM((32, 16, 512), BF16),
            pltpu.VMEM((NY, 5, 16, 512), BF16),
            pltpu.VMEM((3, NY, 16, 512), BF16),
            pltpu.VMEM((16, 1792), F32),
            pltpu.VMEM((512, 1024), BF16),
            pltpu.VMEM((16, 65536), F32),
            pltpu.VMEM((16, 512), F32),
            pltpu.VMEM((16, 256), F32),
            pltpu.VMEM((16, 256), F32),
            pltpu.VMEM((512, 512), BF16),
            pltpu.VMEM((512, 512), BF16),
            pltpu.VMEM((NY, 16, 512), BF16),
            pltpu.VMEM((NY, 16, 128), BF16),
            pltpu.VMEM((8, 64, 128), BF16),
            pltpu.VMEM((8, 64, 128), BF16),
            pltpu.VMEM((NZ, 64, 512), BF16),
            pltpu.VMEM((8, 16, 128), F32),
            pltpu.VMEM((8, NX, 16, 512), BF16),
            pltpu.VMEM((4, 8, 16, 512), BF16),
            pltpu.VMEM((8, NX, 16, 512), BF16),
            pltpu.VMEM((8, NY, 16, 512), BF16),
            pltpu.VMEM((NY, 8, 16, 512), BF16),
            pltpu.VMEM((8, 16, 512), BF16),
            pltpu.VMEM((NZ, 16, 512), BF16),
            dma((9,)), dma, dma((NX,)), dma, dma, dma((8,)), dma((NZ,)), dma, dma((32,)), dma((NZ,)),
            dma((5,)), dma, dma((14,)), dma((2, NZ)), dma, dma((NY,)), dma, dma((3,)),
            dma, dma, dma, dma, dma, dma, dma, dma((NZ,)), dma, dma((32,)), dma, dma,
            dma, dma((4,)), dma, dma((4,)), dma((4,)), dma, dma((4,)), dma, dma,
        ],
        compiler_params=pltpu.CompilerParams(collective_id=0, has_side_effects=True, vmem_limit_bytes=(59 << 20) + (800 << 10)),
        name="layer",
    )(
        hidden_rows, norm_gain, decay_bias, head_gain, mlp_gain, w_query, w_key, w_decay, w_value, w_gate,
        w_out, w_up, w_down, carried_state,
    )
    return flush(out, state)


def solution(mesh):
    finer = Mesh(mesh.devices.reshape(NZ, NY, NX, NC), ("z", "y", "x", "c"))
    placed = (
        P(KV, TP), P(KV, TP), P(), P(KV, TP), P(KV, TP), P(KV, TP), P(KV, TP), P(KV, TP),
        P(TP), P(), P(TP, KV), P(TP), P(TP, KV), P(KV, TP),
    )
    return jax.shard_map(
        body, mesh=finer, in_specs=placed, out_specs=(P(KV, TP), P(KV, TP)), check_vma=False
    )
```
